256 devices in a mesh: fs: 64 (over z, x, core), tp: 4 (over y).
Axes of the slice: x: 4, y: 4, z: 8, core: 2. Of those that a mesh axis runs over, the one named last changes fastest.
Arguments:
- saved_input: bfloat16 [16384, 4096], P('fs'), may hold values from -16 to 16
- query_cotangent: bfloat16 [16384, 2048], P('fs', 'tp'), may hold values from -6 to 6
- layer_cotangent: bfloat16 [16384, 4096], P('fs'), may hold values from -16 to 16
- mixed_heads: bfloat16 [16384, 2048], P('fs', 'tp'), may hold values from -6 to 6
- query_basis: bfloat16 [4096, 256], P('fs'), may hold values from -0.25 to 0.25
- output_basis: bfloat16 [4096, 256], P('fs'), may hold values from -0.25 to 0.25
- query_master: float32 [4096, 2048], P('fs', 'tp'), may hold values from -3 to 3
- output_master: float32 [4096, 2048], P('fs', 'tp'), may hold values from -3 to 3
- query_first: float32 [256, 2048], P('fs', 'tp'), may hold values from -6 to 6
- query_second: float32 [256, 2048], P('fs', 'tp'), may hold values from 0.25 to 4
- output_first: float32 [256, 2048], P('fs', 'tp'), may hold values from -6 to 6
- output_second: float32 [256, 2048], P('fs', 'tp'), may hold values from 0.25 to 4
Outputs:
- query_weight: float32 [4096, 2048], P('fs', 'tp')
- output_weight: float32 [4096, 2048], P('fs', 'tp')
- query_step: float32 [4096, 2048], P('fs', 'tp')
- output_step: float32 [4096, 2048], P('fs', 'tp')
- query_first_new: float32 [256, 2048], P('fs', 'tp')
- query_second_new: float32 [256, 2048], P('fs', 'tp')
- output_first_new: float32 [256, 2048], P('fs', 'tp')
- output_second_new: float32 [256, 2048], P('fs', 'tp')
- query_copy: bfloat16 [4096, 2048], P(None, 'tp')
- output_copy: bfloat16 [4096, 2048], P(None, 'tp')
The draws below stay inside these ranges and needn't reach their ends.
All inputs are finite; a program needn't handle non-finite values.
Results may differ from the reference program's by a relative error of at most 0.0028.
Values may be sent and summed in bfloat16 or wider, within the bound.
No kernel may reach another device: no remote copies, remote signals or barrier semaphores. Data moves between devices by JAX's collectives and lax.ppermute only.
A program may use at most 64 MiB of HBM per device.

```python
import math
import jax
import jax.numpy as jnp
from jax import lax

D = 4096
QW = 2048
RANK = 256
TOKENS = 16384


def with_spikes(values, rng, source, target, parts, factor):
    owner, partner = [(jnp.arange(values.shape[axis_at]) // (values.shape[axis_at] // parts)).reshape([-1 if axis == axis_at else 1 for axis in range(values.ndim)]) for axis_at in (source, target)]
    chosen = jax.random.permutation(rng, parts)[partner]
    strong = (owner == chosen) | (owner == (partner + parts // 2) % parts)
    return jnp.where(strong, factor * values, values)


def block_scale(rng, dims, shards, smallest, high):
    factor_of, own = 1.0, jax.random.fold_in(rng, 6)
    for dim, shards_of in shards:
        draws = jnp.exp(jax.random.uniform(jax.random.fold_in(own, dim), (shards_of,), jnp.float32, smallest / len(shards), high / len(shards)))
        factor_of = factor_of * jnp.repeat(draws, dims[dim] // shards_of).reshape([-1 if axis == dim else 1 for axis in range(len(dims))])
    return factor_of


def centred(stream_key, shape, scale, reach, shards=(), kind=jnp.bfloat16):
    drawn = scale * jax.random.normal(stream_key, shape, jnp.float32)
    if shards:
        drawn = drawn * block_scale(stream_key, shape, shards, -0.22, 0.18)
    return jnp.clip(drawn, -reach, reach).astype(kind)


def bell_draw_with(rng, shape, spread, limit, cuts, heavy, held_as=jnp.bfloat16):
    values = spread * jax.random.normal(rng, shape, jnp.float32)
    if cuts:
        values = values * block_scale(rng, shape, cuts, -0.22, 0.18)
    return jnp.clip(with_spikes(values, jax.random.fold_in(rng, 3), *heavy), -limit, limit).astype(held_as)


def setup_inputs(seed: int = 0) -> dict:
    key_of = jax.random.split(jax.random.key(seed), 13)
    saved_input = bell_draw_with(key_of[0], (TOKENS, D), 1.0, 16.0, ((0, 64),), (0, 1, 64, 4.0))
    query_cotangent = centred(key_of[1], (TOKENS, QW), 1.0, 6.0, ((0, 64), (1, 4)))
    layer_cotangent = bell_draw_with(key_of[2], (TOKENS, D), 1.0, 16.0, ((0, 64),), (0, 1, 64, 4.0))
    mixed_heads = centred(key_of[3], (TOKENS, QW), 1.0, 6.0, ((0, 64), (1, 4)))
    query_basis = bell_draw_with(key_of[4], (D, RANK), D ** -0.5, 0.25, ((0, 64),), (0, 1, 64, 4.0))
    output_basis = bell_draw_with(key_of[5], (D, RANK), D ** -0.5, 0.25, ((0, 64),), (0, 1, 64, 4.0))
    query_master = centred(key_of[6], (D, QW), 0.5, 3.0, ((0, 64), (1, 4)), jnp.float32)
    output_master = centred(key_of[7], (D, QW), 0.5, 3.0, ((0, 64), (1, 4)), jnp.float32)
    query_first = centred(key_of[8], (RANK, QW), 1.0, 6.0, ((0, 64), (1, 4)), jnp.float32)
    query_second = jnp.clip(jnp.exp(math.log(4.0) - 2.7725887 * jax.random.uniform(key_of[9], (RANK, QW), jnp.float32) ** block_scale(key_of[9], (RANK, QW), ((0, 64), (1, 4)), -0.2, 0.2)), 0.25, 4.0)
    output_first = centred(key_of[10], (RANK, QW), 1.0, 6.0, ((0, 64), (1, 4)), jnp.float32)
    output_second = jnp.clip(jnp.exp(math.log(4.0) - 2.7725887 * jax.random.uniform(key_of[11], (RANK, QW), jnp.float32) ** block_scale(key_of[11], (RANK, QW), ((0, 64), (1, 4)), -0.2, 0.2)), 0.25, 4.0)
    return dict(saved_input=saved_input, query_cotangent=query_cotangent, layer_cotangent=layer_cotangent, mixed_heads=mixed_heads, query_basis=query_basis, output_basis=output_basis, query_master=query_master, output_master=output_master, query_first=query_first, query_second=query_second, output_first=output_first, output_second=output_second)


beta_one = 0.8
beta_two = 0.9
rate = 0.1

def projected_gradient(saved, cotangent, basis):
    gradient = jnp.dot(saved.T, cotangent, preferred_element_type=jnp.float32)
    return jnp.dot(basis.astype(jnp.float32).T, gradient, precision=lax.Precision.HIGHEST)

def moment_update(low, factor, first, second):
    scaled = low * factor
    first_new = beta_one * first + (1.0 - beta_one) * scaled
    second_new = beta_two * second + (1.0 - beta_two) * scaled * scaled
    direction = (first_new / jnp.sqrt(second_new)).astype(jnp.bfloat16)
    return (first_new, second_new, direction)

def reference(saved_input, query_cotangent, layer_cotangent, mixed_heads, query_basis, output_basis, query_master, output_master, query_first, query_second, output_first, output_second):
    query_low = projected_gradient(saved_input, query_cotangent, query_basis)
    output_low = projected_gradient(layer_cotangent, mixed_heads, output_basis)
    meansq = (jnp.sum(query_low * query_low) + jnp.sum(output_low * output_low)) / (2.0 * RANK * QW)
    factor = 1.0 / jnp.sqrt(1.0 + meansq)
    qf, qs, qdir = moment_update(query_low, factor, query_first, query_second)
    of, osec, odir = moment_update(output_low, factor, output_first, output_second)
    query_step = jnp.dot(query_basis, qdir, preferred_element_type=jnp.float32)
    output_step = jnp.dot(output_basis, odir, preferred_element_type=jnp.float32)
    query_weight = query_master - rate * query_step
    output_weight = output_master - rate * output_step
    return (query_weight, output_weight, query_step, output_step, qf, qs, of, osec, query_weight.astype(jnp.bfloat16), output_weight.astype(jnp.bfloat16))
```

```python
import jax
import jax.numpy as jnp
from jax import lax
from jax.experimental import pallas as pl
from jax.experimental.pallas import tpu as pltpu
from jax.sharding import Mesh
from jax.sharding import PartitionSpec as P

D = 4096
QW = 2048
RANK = 256
FS = ("fs_0", "fs_1", "fs_2")
CHIPS = ("fs_0", "fs_1")

beta_one = 0.8
beta_two = 0.9
rate = 0.1

f32 = jnp.float32
bf16 = jnp.bfloat16
f16 = jnp.float16

SPAN = 248.0
SHRINK = 2.0**-9

MASTER_ROWS = 128
BASIS_ROWS = 64
TOP_ROWS = 8
HEAD_ROWS = MASTER_ROWS + BASIS_ROWS + TOP_ROWS
MOMENT_ROWS = 32
BLOCK_ROWS = HEAD_ROWS + MOMENT_ROWS
GROUP = 8


def split_in_two(values):
    high = values.astype(bf16)
    return high, (values - high.astype(f32)).astype(bf16)


def top_of(values):
    return (jnp.max(jnp.abs(values)) * 1.01 + 1e-30).astype(bf16)


def coded(values, top):
    level = jnp.exp2(jnp.abs(values) * (SPAN / top.astype(f32)) - SPAN / 2)
    return jnp.where(values < 0, -level, level).astype(bf16)


def decoded(codes, top):
    level = (jnp.log2(jnp.abs(codes)) + SPAN / 2) * (top / SPAN)
    return jnp.where(codes < 0, -level, level)


def copies_kernel(block, direction, query_copy, output_copy):
    half = direction.shape[1] // 2
    basis = block[:, MASTER_ROWS : MASTER_ROWS + BASIS_ROWS, :].reshape(GROUP * BASIS_ROWS, 2 * RANK)
    tops = block[:, MASTER_ROWS + BASIS_ROWS :, :].astype(f32)
    for out, side in ((query_copy, 0), (output_copy, 1)):
        step = jnp.dot(
            basis[:, side * RANK : (side + 1) * RANK],
            direction[:, side * half : (side + 1) * half],
            preferred_element_type=f32,
        ).reshape(GROUP, 64, half)
        codes = block[:, side * 64 : (side + 1) * 64, :].astype(f32)
        top = tops[:, side : side + 1, :]
        out[...] = (decoded(codes, top) - rate * step).astype(bf16).reshape(GROUP * 64, half)


def copies_of(gathered, direction):
    fs = gathered.shape[0]
    half = direction.shape[1] // 2
    out = jax.ShapeDtypeStruct((fs * 64, half), bf16)
    return pl.pallas_call(
        copies_kernel,
        grid=(fs // GROUP,),
        in_specs=[
            pl.BlockSpec((GROUP, HEAD_ROWS, gathered.shape[2]), lambda i: (i, 0, 0)),
            pl.BlockSpec(direction.shape, lambda i: (0, 0)),
        ],
        out_specs=[pl.BlockSpec((GROUP * 64, half), lambda i: (i, 0))] * 2,
        out_shape=[out, out],
        compiler_params=pltpu.CompilerParams(dimension_semantics=("arbitrary",)),
        name="copies",
    )(gathered, direction)


def moment_update(low, factor, first, second):
    scaled = low * factor
    first_new = beta_one * first + (1.0 - beta_one) * scaled
    second_new = beta_two * second + (1.0 - beta_two) * scaled * scaled
    direction = (first_new / jnp.sqrt(second_new)).astype(bf16)
    return first_new, second_new, direction


def shifted(values, axis, by):
    peers = lax.axis_size(axis)
    return lax.ppermute(values, axis, [(i, (i + by) % peers) for i in range(peers)])


def contract_tokens(left, right):
    return lax.dot_general(left, right, (((0,), (0,)), ((), ())), preferred_element_type=f32)


def per_device(
    saved_input,
    query_cotangent,
    layer_cotangent,
    mixed_heads,
    query_basis,
    output_basis,
    query_master,
    output_master,
    query_first,
    query_second,
    output_first,
    output_second,
):
    at_tp = lax.axis_index("tp")
    at_core = lax.axis_index("fs_2")
    fs, tp = lax.axis_size(FS), lax.axis_size("tp")
    chips = fs // 2
    quarter = RANK // tp
    width = QW // tp
    query_top, output_top = top_of(query_master), top_of(output_master)
    moments = []
    for values in (query_first, query_second, output_first, output_second):
        moments.extend(split_in_two(values))
    tops = jnp.stack([query_top, output_top])[:, None] * jnp.ones((1, width), bf16)
    block = jnp.concatenate(
        [
            coded(query_master, query_top),
            coded(output_master, output_top),
            jnp.concatenate([query_basis, output_basis], axis=1),
            jnp.pad(tops, ((0, TOP_ROWS - 2), (0, 0))),
            *moments,
        ],
        axis=0,
    )
    block, query_basis, output_basis = lax.optimization_barrier((block, query_basis, output_basis))
    gathered = lax.all_gather(block, FS, axis=0, tiled=False)

    cotangent = jnp.concatenate([query_cotangent, mixed_heads], axis=1)
    cotangents = [cotangent] + [shifted(cotangent, "tp", k) for k in range(1, tp)]

    mine = jnp.concatenate(
        [
            lax.dynamic_slice_in_dim(query_basis, at_tp * quarter, quarter, axis=1),
            lax.dynamic_slice_in_dim(output_basis, at_tp * quarter, quarter, axis=1),
        ],
        axis=1,
    )
    mine = lax.all_to_all(jnp.broadcast_to(mine[None], (chips, *mine.shape)), CHIPS, 0, 0, tiled=True)
    theirs = shifted(mine, "fs_2", 1)
    first_core = jnp.where(at_core == 0, mine, theirs)
    second_core = jnp.where(at_core == 0, theirs, mine)
    basis = jnp.stack([first_core, second_core], axis=1).reshape(D, 2 * quarter)

    query_coords = jnp.dot(saved_input, basis, preferred_element_type=f32)[:, :quarter]
    output_coords = jnp.dot(layer_cotangent, basis, preferred_element_type=f32)[:, quarter:]
    parts = []
    for side, coords in ((0, query_coords), (1, output_coords)):
        high, low = split_in_two(coords)
        for values in cotangents:
            right = values[:, side * width : (side + 1) * width]
            parts.append(contract_tokens(high, right) + contract_tokens(low, right))
    partial = (jnp.stack(parts, axis=1) * SHRINK).astype(f16).reshape(fs, 2 * QW // 128, 128)
    arrived = lax.all_to_all(partial, FS, 0, 0, tiled=True)
    row = jnp.sum(arrived.astype(f32), axis=0) * (1.0 / SHRINK)
    squares = jnp.sum(row * row)
    row = row.reshape(2, tp, width)
    order = (at_tp - jnp.arange(tp)) % tp
    row = jnp.take(row, order, axis=1)
    out = jnp.concatenate(
        [jnp.moveaxis(row, 1, 0).reshape(tp, 2 * width), jnp.full((tp, 128), squares, f32)], axis=1
    )
    out = jnp.broadcast_to(out[None], (chips, *out.shape)).reshape(chips * tp, 1, 2 * width + 128)
    mine = lax.all_to_all(out, (*CHIPS, "tp"), 0, 0, tiled=True)
    theirs = shifted(mine, "fs_2", 1)
    total = jnp.sum(mine[:, 0, 2 * width]) + jnp.sum(theirs[:, 0, 2 * width])
    factor = 1.0 / jnp.sqrt(1.0 + total / (2.0 * RANK * QW))
    mine = mine[:, 0, : 2 * width].reshape(chips, tp, 2 * width)
    theirs = theirs[:, 0, : 2 * width].reshape(chips, tp, 2 * width)
    low = jnp.stack(
        [jnp.where(at_core == 0, mine, theirs), jnp.where(at_core == 0, theirs, mine)], axis=1
    )
    low = jnp.moveaxis(low, 2, 0).reshape(RANK, 2 * width)

    at_fs = lax.axis_index(FS)
    own = lax.dynamic_slice_in_dim(low, at_fs * (RANK // fs), RANK // fs, axis=0)
    qf, qs, _ = moment_update(own[:, :width], factor, query_first, query_second)
    of, osec, _ = moment_update(own[:, width:], factor, output_first, output_second)

    kept = gathered[:, HEAD_ROWS:].reshape(fs, 4, 2, RANK // fs, width).astype(f32).sum(axis=2)
    kept = jnp.moveaxis(kept, 1, 0).reshape(4, RANK, width)
    query_direction = moment_update(low[:, :width], factor, kept[0], kept[1])[2]
    output_direction = moment_update(low[:, width:], factor, kept[2], kept[3])[2]
    query_step = jnp.dot(query_basis, query_direction, preferred_element_type=f32)
    output_step = jnp.dot(output_basis, output_direction, preferred_element_type=f32)
    query_copy, output_copy = copies_of(gathered, jnp.concatenate([query_direction, output_direction], axis=1))
    return (
        query_master - rate * query_step,
        output_master - rate * output_step,
        query_step,
        output_step,
        qf,
        qs,
        of,
        osec,
        query_copy,
        output_copy,
    )


def solution(mesh):
    torus = Mesh(mesh.devices.reshape(8, 4, 2, mesh.shape["tp"]), (*FS, "tp"))
    return jax.shard_map(
        per_device,
        mesh=torus,
        in_specs=(
            P(FS, None),
            P(FS, "tp"),
            P(FS, None),
            P(FS, "tp"),
            P(FS, None),
            P(FS, None),
            *[P(FS, "tp")] * 6,
        ),
        out_specs=(*[P(FS, "tp")] * 8, P(None, "tp"), P(None, "tp")),
        check_vma=False,
    )
```

```python
import jax
import jax.numpy as jnp
from jax import lax
from jax.experimental import pallas as pl
from jax.experimental.pallas import tpu as pltpu
from jax.sharding import Mesh
from jax.sharding import PartitionSpec as P

D = 4096
QW = 2048
RANK = 256
FS = ("fs_0", "fs_1", "fs_2")
CHIPS = ("fs_0", "fs_1")

beta_one = 0.8
beta_two = 0.9
rate = 0.1

f32 = jnp.float32
bf16 = jnp.bfloat16
f16 = jnp.float16

REACH = 85.0
SHRINK = 2.0**-10

MOMENTS_AT = 192
TOPS_AT = 224
BLOCK_ROWS = 232
GROUP = 8


VMEM = pl.BlockSpec(memory_space=pltpu.VMEM)
SMEM = pl.BlockSpec(memory_space=pltpu.SMEM)


def high_and_low(values):
    high = values.astype(bf16).astype(f32)
    return high, values - high


def pack_kernel(at, qb, ob, qm, om, q1, q2, o1, o2, qc, oc, block, send, cot):
    tp = at[1]
    picked = []
    for basis in (qb, ob):
        full = basis[...].astype(f32)
        part = full[:, :64]
        for t in range(1, 4):
            part = jnp.where(tp == t, full[:, 64 * t : 64 * t + 64], part)
        picked.append(part)
    send[...] = jnp.broadcast_to(jnp.concatenate(picked, axis=1).astype(bf16)[None], send.shape)
    tops = []
    for side, master in ((0, qm), (1, om)):
        values = master[...]
        top = jnp.max(jnp.abs(values), axis=(0, 1), keepdims=True) * 1.01 + 1e-30
        top = top.astype(bf16).astype(f32)
        block[64 * side : 64 * side + 64, :] = jnp.exp(values * (REACH / top)).astype(bf16)
        tops.append(top)
    block[128:192, :256] = qb[...]
    block[128:192, 256:] = ob[...]
    for side, (first, second) in enumerate(((q1, q2), (o1, o2))):
        first_high, first_low = high_and_low(first[...])
        second_high, second_low = high_and_low(second[...])
        at_row = MOMENTS_AT + 16 * side
        block[at_row : at_row + 16, :] = jnp.concatenate(
            [first_high, second_high, first_low, second_low], axis=0
        ).astype(bf16)
    row = lax.broadcasted_iota(jnp.int32, (8, 512), 0)
    block[TOPS_AT:, :] = jnp.where(row == 0, tops[0], tops[1]).astype(bf16)
    cot[:, :512] = qc[...]
    cot[:, 512:] = oc[...]


def project_kernel(at, saved, layer, mine, theirs, c0, c1, c2, c3, keep, give):
    core = at[0]
    own, other = mine[...], theirs[...]
    first = jnp.where(core == 0, own, other)
    second = jnp.where(core == 0, other, own)
    basis = jnp.concatenate([first, second], axis=1).reshape(D, 128)
    for side, source in ((0, saved), (1, layer)):
        coords = jnp.dot(source[...], basis, preferred_element_type=f32)[:, 64 * side : 64 * side + 64]
        high, low = high_and_low(coords.T)
        left = jnp.concatenate([high, low], axis=0).astype(bf16)
        for k, cot in enumerate((c0, c1, c2, c3)):
            both = jnp.dot(left, cot[:, 512 * side : 512 * side + 512], preferred_element_type=f32)
            part = (both[:64] + both[64:]) * SHRINK
            lower, upper = part[:32], part[32:]
            kept = jnp.where(core == 0, lower, upper)
            given = jnp.where(core == 0, upper, lower)
            for j in range(4):
                slot = (side * 4 + k) * 4 + j
                keep[:, slot, :] = kept[:, 128 * j : 128 * j + 128]
                give[:, slot, :] = given[:, 128 * j : 128 * j + 128]


def spread_kernel(at, row, out):
    tp = at[1]
    values = row[...] * (1.0 / SHRINK)
    squares = jnp.broadcast_to(jnp.sum(values * values, axis=(0, 1), keepdims=True), (1, 128))
    for t in range(4):
        k = (tp + 4 - t) % 4
        pieces = []
        for side in range(2):
            for j in range(4):
                pieces.append(row[pl.ds((side * 4 + k) * 4 + j, 1), :] * (1.0 / SHRINK))
        line = jnp.concatenate(pieces + [squares], axis=1)

        def put(chip, carry):
            out[chip * 4 + t] = line
            return carry

        lax.fori_loop(0, 32, put, 0, unroll=True)


def update_kernel(at, mine, theirs, q1, q2, o1, o2, low, factor, qf, qs, of, os):
    core, fs = at[0], at[2]
    total = jnp.sum(mine[:, :, 1024:], axis=0) + jnp.sum(theirs[:, :, 1024:], axis=0)
    scale = lax.rsqrt(1.0 + total * (1.0 / (2.0 * RANK * QW)))
    factor[...] = jnp.broadcast_to(scale, (8, 128))
    is_first = core == 0
    for t in range(4):
        for chip in range(32):
            own, other = mine[chip * 4 + t, :, :1024], theirs[chip * 4 + t, :, :1024]
            low[64 * t + chip : 64 * t + chip + 1, :] = jnp.where(is_first, own, other)
            low[64 * t + 32 + chip : 64 * t + 33 + chip, :] = jnp.where(is_first, other, own)
    near = low[pl.ds(pl.multiple_of(fs // 2 * 8, 8), 8), :]
    own_rows = jnp.where(fs % 2 == 0, near[:4], near[4:]) * scale[:, :1]
    for side, first, second, first_new, second_new in ((0, q1, q2, qf, qs), (1, o1, o2, of, os)):
        scaled = own_rows[:, 512 * side : 512 * side + 512]
        first_new[...] = beta_one * first[...] + (1.0 - beta_one) * scaled
        second_new[...] = beta_two * second[...] + (1.0 - beta_two) * scaled * scaled


def finish_kernel(factor, low, qb, ob, qm, om, moments, block, tops, qw, ow, qs, os, qc, oc, direction):
    @pl.when(pl.program_id(0) == 0)
    def _():
        scale = factor[0:1, 0:1]

        def rows(i, carry):
            held = moments[pl.ds(4 * i, 4)].astype(f32)
            lows = low[pl.ds(16 * i, 16), :] * scale
            for side in range(2):
                sums = [held[j, 16 * side : 16 * side + 8] + held[j, 16 * side + 8 : 16 * side + 16] for j in range(4)]
                first = jnp.concatenate([s[:4] for s in sums], axis=0)
                second = jnp.concatenate([s[4:] for s in sums], axis=0)
                scaled = lows[:, 512 * side : 512 * side + 512]
                first = beta_one * first + (1.0 - beta_one) * scaled
                second = beta_two * second + (1.0 - beta_two) * scaled * scaled
                direction[pl.ds(16 * i, 16), 512 * side : 512 * side + 512] = (first / jnp.sqrt(second)).astype(bf16)
            return carry

        lax.fori_loop(0, 16, rows, 0)
        for side, basis, master, weight, step in ((0, qb, qm, qw, qs), (1, ob, om, ow, os)):
            moved = jnp.dot(basis[...], direction[:, 512 * side : 512 * side + 512], preferred_element_type=f32)
            step[...] = moved
            weight[...] = master[...] - rate * moved

    for side, copy in ((0, qc), (1, oc)):
        basis = block[:, 128:192, 256 * side : 256 * side + 256].reshape(GROUP * 64, 256)
        moved = jnp.dot(basis, direction[:, 512 * side : 512 * side + 512], preferred_element_type=f32)
        codes = block[:, 64 * side : 64 * side + 64, :].astype(f32)
        unit = tops[:, side : side + 1, :].astype(f32) * (1.0 / REACH)
        master = (jnp.log(codes) * unit).reshape(GROUP * 64, 512)
        copy[...] = (master - rate * moved).astype(bf16)


def swapped(values):
    return lax.ppermute(values, "fs_2", [(0, 1), (1, 0)])


def per_device(
    saved_input,
    query_cotangent,
    layer_cotangent,
    mixed_heads,
    query_basis,
    output_basis,
    query_master,
    output_master,
    query_first,
    query_second,
    output_first,
    output_second,
):
    shape = jax.ShapeDtypeStruct
    at = jnp.stack([lax.axis_index("fs_2"), lax.axis_index("tp"), lax.axis_index(FS)]).astype(jnp.int32)
    moments = (query_first, query_second, output_first, output_second)
    block, send, cot = pl.pallas_call(
        pack_kernel,
        in_specs=[SMEM] + [VMEM] * 10,
        out_specs=[VMEM] * 3,
        out_shape=[shape((BLOCK_ROWS, 512), bf16), shape((32, 64, 128), bf16), shape((256, 1024), bf16)],
        name="pack",
    )(at, query_basis, output_basis, query_master, output_master, *moments, query_cotangent, mixed_heads)
    gathered = lax.all_gather(block, FS, axis=0, tiled=False)
    cots = [cot] + [lax.ppermute(cot, "tp", [(i, (i + k) % 4) for i in range(4)]) for k in range(1, 4)]
    mine = lax.all_to_all(send, CHIPS, 0, 0, tiled=True)
    theirs = swapped(mine)
    keep, give = pl.pallas_call(
        project_kernel,
        in_specs=[SMEM] + [VMEM] * 8,
        out_specs=[VMEM] * 2,
        out_shape=[shape((32, 32, 128), f32)] * 2,
        name="project",
    )(at, saved_input, layer_cotangent, mine, theirs, *cots)
    pair = (keep + swapped(give.astype(f16)).astype(f32)).astype(f16)
    arrived = lax.all_to_all(pair, CHIPS, 0, 0, tiled=True)
    row = jnp.sum(arrived.astype(f32), axis=0)
    out = pl.pallas_call(
        spread_kernel,
        in_specs=[SMEM, VMEM],
        out_specs=VMEM,
        out_shape=shape((128, 1, 1152), f32),
        name="spread",
    )(at, row)
    mine = lax.all_to_all(out, (*CHIPS, "tp"), 0, 0, tiled=True)
    theirs = swapped(mine)
    low, factor, qf, qs, of, osec = pl.pallas_call(
        update_kernel,
        in_specs=[SMEM] + [VMEM] * 6,
        out_specs=[VMEM] * 6,
        out_shape=[shape((RANK, 1024), f32), shape((8, 128), f32)] + [shape((4, 512), f32)] * 4,
        name="update",
    )(at, mine, theirs, *moments)

    def whole(*dims):
        return pl.BlockSpec(dims, lambda i: (0,) * len(dims))

    local = whole(64, 512)
    query_weight, output_weight, query_step, output_step, query_copy, output_copy = pl.pallas_call(
        finish_kernel,
        grid=(64 // GROUP,),
        in_specs=[
            whole(8, 128),
            whole(RANK, 1024),
            whole(64, 256),
            whole(64, 256),
            local,
            local,
            pl.BlockSpec((64, 32, 512), lambda i: (0, MOMENTS_AT // 32, 0)),
            pl.BlockSpec((GROUP, 192, 512), lambda i: (i, 0, 0)),
            pl.BlockSpec((GROUP, 8, 512), lambda i: (i, TOPS_AT // 8, 0)),
        ],
        out_specs=[local] * 4 + [pl.BlockSpec((GROUP * 64, 512), lambda i: (i, 0))] * 2,
        out_shape=[shape((64, 512), f32)] * 4 + [shape((D, 512), bf16)] * 2,
        scratch_shapes=[pltpu.VMEM((RANK, 1024), bf16)],
        compiler_params=pltpu.CompilerParams(dimension_semantics=("arbitrary",)),
        name="finish",
    )(factor, low, query_basis, output_basis, query_master, output_master, gathered, gathered, gathered)
    return (
        query_weight,
        output_weight,
        query_step,
        output_step,
        qf,
        qs,
        of,
        osec,
        query_copy,
        output_copy,
    )


def solution(mesh):
    torus = Mesh(mesh.devices.reshape(8, 4, 2, mesh.shape["tp"]), (*FS, "tp"))
    return jax.shard_map(
        per_device,
        mesh=torus,
        in_specs=(
            P(FS, None),
            P(FS, "tp"),
            P(FS, None),
            P(FS, "tp"),
            P(FS, None),
            P(FS, None),
            *[P(FS, "tp")] * 6,
        ),
        out_specs=(*[P(FS, "tp")] * 8, P(None, "tp"), P(None, "tp")),
        check_vma=False,
    )
```

```python
import jax
import jax.numpy as jnp
from jax import lax
from jax.experimental import pallas as pl
from jax.experimental.pallas import tpu as pltpu
from jax.sharding import Mesh
from jax.sharding import PartitionSpec as P

D = 4096
QW = 2048
RANK = 256
FS = ("fs_0", "fs_1", "fs_2")
CHIPS = ("fs_0", "fs_1")

beta_one = 0.8
beta_two = 0.9
rate = 0.1

f32 = jnp.float32
bf16 = jnp.bfloat16
f16 = jnp.float16

REACH = 85.0
SHRINK = 2.0**-10

MOMENTS_AT = 192
TOPS_AT = 224
BLOCK_ROWS = 232
GROUP = 4


VMEM = pl.BlockSpec(memory_space=pltpu.VMEM)
SMEM = pl.BlockSpec(memory_space=pltpu.SMEM)


def high_and_low(values):
    high = values.astype(bf16).astype(f32)
    return high, values - high


def pack_kernel(at, qb, ob, qm, om, q1, q2, o1, o2, qc, oc, block, send, cot):
    tp = at[1]
    picked = []
    for basis in (qb, ob):
        full = basis[...].astype(f32)
        part = full[:, :64]
        for t in range(1, 4):
            part = jnp.where(tp == t, full[:, 64 * t : 64 * t + 64], part)
        picked.append(part)
    send[...] = jnp.broadcast_to(jnp.concatenate(picked, axis=1).astype(bf16)[None], send.shape)
    tops = []
    for side, master in ((0, qm), (1, om)):
        values = master[...]
        top = jnp.max(jnp.abs(values), axis=(0, 1), keepdims=True) * 1.01 + 1e-30
        top = top.astype(bf16).astype(f32)
        block[64 * side : 64 * side + 64, :] = jnp.exp(values * (REACH / top)).astype(bf16)
        tops.append(top)
    block[128:192, :256] = qb[...]
    block[128:192, 256:] = ob[...]
    for side, (first, second) in enumerate(((q1, q2), (o1, o2))):
        first_high, first_low = high_and_low(first[...])
        second_high, second_low = high_and_low(second[...])
        at_row = MOMENTS_AT + 16 * side
        block[at_row : at_row + 16, :] = jnp.concatenate(
            [first_high, second_high, first_low, second_low], axis=0
        ).astype(bf16)
    row = lax.broadcasted_iota(jnp.int32, (8, 512), 0)
    block[TOPS_AT:, :] = jnp.where(row == 0, tops[0], tops[1]).astype(bf16)
    cot[:, :512] = qc[...]
    cot[:, 512:] = oc[...]


def project_kernel(at, saved, layer, mine, theirs, c0, c1, c2, c3, keep, give, saved_near, layer_near, sems):
    copies = [
        pltpu.make_async_copy(saved, saved_near, sems.at[0]),
        pltpu.make_async_copy(layer, layer_near, sems.at[1]),
    ]
    for copy in copies:
        copy.start()
    core = at[0]
    own, other = mine[...], theirs[...]
    first = jnp.where(core == 0, own, other)
    second = jnp.where(core == 0, other, own)
    basis = jnp.concatenate([first, second], axis=1).reshape(D, 128)
    for side, source in ((0, saved_near), (1, layer_near)):
        copies[side].wait()
        coords = jnp.dot(source[...], basis, preferred_element_type=f32)[:, 64 * side : 64 * side + 64]
        high, low = high_and_low(coords.T)
        left = jnp.concatenate([high, low], axis=0).astype(bf16)
        for k, cot in enumerate((c0, c1, c2, c3)):
            both = jnp.dot(left, cot[:, 512 * side : 512 * side + 512], preferred_element_type=f32)
            part = (both[:64] + both[64:]) * SHRINK
            lower, upper = part[:32], part[32:]
            kept = jnp.where(core == 0, lower, upper)
            given = jnp.where(core == 0, upper, lower)
            for j in range(4):
                slot = (side * 4 + k) * 4 + j
                keep[:, slot, :] = kept[:, 128 * j : 128 * j + 128]
                give[:, slot, :] = given[:, 128 * j : 128 * j + 128]


def spread_kernel(at, row, out):
    tp = at[1]
    values = row[...] * (1.0 / SHRINK)
    squares = jnp.broadcast_to(jnp.sum(values * values, axis=(0, 1), keepdims=True), (1, 128))
    for t in range(4):
        k = (tp + 4 - t) % 4
        pieces = []
        for side in range(2):
            for j in range(4):
                pieces.append(row[pl.ds((side * 4 + k) * 4 + j, 1), :] * (1.0 / SHRINK))
        line = jnp.concatenate(pieces + [squares], axis=1)

        def put(chip, carry):
            out[chip * 4 + t] = line
            return carry

        lax.fori_loop(0, 32, put, 0, unroll=True)


def update_kernel(at, mine, theirs, q1, q2, o1, o2, low, factor, qf, qs, of, os):
    core, fs = at[0], at[2]
    total = jnp.sum(mine[:, :, 1024:], axis=0) + jnp.sum(theirs[:, :, 1024:], axis=0)
    scale = lax.rsqrt(1.0 + total * (1.0 / (2.0 * RANK * QW)))
    factor[...] = jnp.broadcast_to(scale, (8, 128))
    is_first = core == 0
    for t in range(4):
        for chip in range(32):
            own, other = mine[chip * 4 + t, :, :1024], theirs[chip * 4 + t, :, :1024]
            low[64 * t + chip : 64 * t + chip + 1, :] = jnp.where(is_first, own, other)
            low[64 * t + 32 + chip : 64 * t + 33 + chip, :] = jnp.where(is_first, other, own)
    near = low[pl.ds(pl.multiple_of(fs // 2 * 8, 8), 8), :]
    own_rows = jnp.where(fs % 2 == 0, near[:4], near[4:]) * scale[:, :1]
    for side, first, second, first_new, second_new in ((0, q1, q2, qf, qs), (1, o1, o2, of, os)):
        scaled = own_rows[:, 512 * side : 512 * side + 512]
        first_new[...] = beta_one * first[...] + (1.0 - beta_one) * scaled
        second_new[...] = beta_two * second[...] + (1.0 - beta_two) * scaled * scaled


def finish_kernel(factor, low, qb, ob, qm, om, moments, block, tops, qw, ow, qs, os, qc, oc, direction):
    @pl.when(pl.program_id(0) == 0)
    def _():
        scale = factor[0:1, 0:1]

        def rows(i, carry):
            held = moments[pl.ds(4 * i, 4)].astype(f32)
            lows = low[pl.ds(16 * i, 16), :] * scale
            for side in range(2):
                sums = [held[j, 16 * side : 16 * side + 8] + held[j, 16 * side + 8 : 16 * side + 16] for j in range(4)]
                first = jnp.concatenate([s[:4] for s in sums], axis=0)
                second = jnp.concatenate([s[4:] for s in sums], axis=0)
                scaled = lows[:, 512 * side : 512 * side + 512]
                first = beta_one * first + (1.0 - beta_one) * scaled
                second = beta_two * second + (1.0 - beta_two) * scaled * scaled
                direction[pl.ds(16 * i, 16), 512 * side : 512 * side + 512] = (first / jnp.sqrt(second)).astype(bf16)
            return carry

        lax.fori_loop(0, 16, rows, 0)
        for side, basis, master, weight, step in ((0, qb, qm, qw, qs), (1, ob, om, ow, os)):
            moved = jnp.dot(basis[...], direction[:, 512 * side : 512 * side + 512], preferred_element_type=f32)
            step[...] = moved
            weight[...] = master[...] - rate * moved

    for side, copy in ((0, qc), (1, oc)):
        basis = block[:, 128:192, 256 * side : 256 * side + 256].reshape(GROUP * 64, 256)
        moved = jnp.dot(basis, direction[:, 512 * side : 512 * side + 512], preferred_element_type=f32)
        codes = block[:, 64 * side : 64 * side + 64, :].astype(f32)
        unit = tops[:, side : side + 1, :].astype(f32) * (1.0 / REACH)
        master = (jnp.log(codes) * unit).reshape(GROUP * 64, 512)
        copy[...] = (master - rate * moved).astype(bf16)


def near(*arrays):
    return [pltpu.with_memory_space_constraint(a, pltpu.VMEM) for a in arrays]


def far(*arrays):
    return [pltpu.with_memory_space_constraint(a, pltpu.HBM) for a in arrays]


def swapped(values):
    return lax.ppermute(values, "fs_2", [(0, 1), (1, 0)])


def per_device(
    saved_input,
    query_cotangent,
    layer_cotangent,
    mixed_heads,
    query_basis,
    output_basis,
    query_master,
    output_master,
    query_first,
    query_second,
    output_first,
    output_second,
):
    shape = jax.ShapeDtypeStruct
    at = jnp.stack([lax.axis_index("fs_2"), lax.axis_index("tp"), lax.axis_index(FS)]).astype(jnp.int32)
    moments = (query_first, query_second, output_first, output_second)
    block, send, cot = pl.pallas_call(
        pack_kernel,
        in_specs=[SMEM] + [VMEM] * 10,
        out_specs=[VMEM] * 3,
        out_shape=[shape((BLOCK_ROWS, 512), bf16), shape((32, 64, 128), bf16), shape((256, 1024), bf16)],
        compiler_params=pltpu.CompilerParams(vmem_limit_bytes=24 * 2**20),
        name="pack",
    )(
        at,
        *far(query_basis, output_basis, query_master, output_master, *moments),
        *far(query_cotangent, mixed_heads),
    )
    gathered = lax.all_gather(block, FS, axis=0, tiled=False)
    cots = [cot] + [lax.ppermute(cot, "tp", [(i, (i + k) % 4) for i in range(4)]) for k in (2, 1, 3)]
    cots = [cots[i] for i in (0, 2, 1, 3)]
    mine = lax.all_to_all(send, CHIPS, 0, 0, tiled=True)
    theirs = swapped(mine)
    keep, give = pl.pallas_call(
        project_kernel,
        in_specs=[SMEM] + [pl.BlockSpec(memory_space=pl.ANY)] * 2 + [VMEM] * 6,
        out_specs=[VMEM] * 2,
        scratch_shapes=[pltpu.VMEM((256, D), bf16)] * 2 + [pltpu.SemaphoreType.DMA((2,))],
        out_shape=[pltpu.VMEM((32, 32, 128), f32)] * 2,
        compiler_params=pltpu.CompilerParams(vmem_limit_bytes=20 * 2**20),
        name="project",
    )(at, *far(saved_input, layer_cotangent), *near(mine, theirs, *cots))
    pair = (keep + swapped(give.astype(f16)).astype(f32)).astype(f16)
    arrived = lax.all_to_all(pair, CHIPS, 0, 0, tiled=True)
    row = jnp.sum(arrived.astype(f32), axis=0)
    out = pl.pallas_call(
        spread_kernel,
        in_specs=[SMEM, VMEM],
        out_specs=VMEM,
        out_shape=pltpu.VMEM((128, 1, 1152), f32),
        compiler_params=pltpu.CompilerParams(vmem_limit_bytes=16 * 2**20),
        name="spread",
    )(at, *near(row))
    mine = lax.all_to_all(out, (*CHIPS, "tp"), 0, 0, tiled=True)
    theirs = swapped(mine)
    low, factor, qf, qs, of, osec = pl.pallas_call(
        update_kernel,
        in_specs=[SMEM] + [VMEM] * 6,
        out_specs=[VMEM] * 6,
        out_shape=[shape((RANK, 1024), f32), shape((8, 128), f32)] + [shape((4, 512), f32)] * 4,
        compiler_params=pltpu.CompilerParams(vmem_limit_bytes=16 * 2**20),
        name="update",
    )(at, *near(mine, theirs), *far(*moments))

    def whole(*dims):
        return pl.BlockSpec(dims, lambda i: (0,) * len(dims))

    local = whole(64, 512)
    query_weight, output_weight, query_step, output_step, query_copy, output_copy = pl.pallas_call(
        finish_kernel,
        grid=(64 // GROUP,),
        in_specs=[
            whole(8, 128),
            whole(RANK, 1024),
            whole(64, 256),
            whole(64, 256),
            local,
            local,
            pl.BlockSpec((64, 32, 512), lambda i: (0, MOMENTS_AT // 32, 0)),
            pl.BlockSpec((GROUP, 192, 512), lambda i: (i, 0, 0)),
            pl.BlockSpec((GROUP, 8, 512), lambda i: (i, TOPS_AT // 8, 0)),
        ],
        out_specs=[local] * 4 + [pl.BlockSpec((GROUP * 64, 512), lambda i: (i, 0))] * 2,
        out_shape=[shape((64, 512), f32)] * 4 + [shape((D, 512), bf16)] * 2,
        scratch_shapes=[pltpu.VMEM((RANK, 1024), bf16)],
        compiler_params=pltpu.CompilerParams(dimension_semantics=("arbitrary",)),
        name="finish",
    )(factor, low, query_basis, output_basis, query_master, output_master, gathered, gathered, gathered)
    return (
        query_weight,
        output_weight,
        query_step,
        output_step,
        qf,
        qs,
        of,
        osec,
        query_copy,
        output_copy,
    )


def solution(mesh):
    torus = Mesh(mesh.devices.reshape(8, 4, 2, mesh.shape["tp"]), (*FS, "tp"))
    return jax.shard_map(
        per_device,
        mesh=torus,
        in_specs=(
            P(FS, None),
            P(FS, "tp"),
            P(FS, None),
            P(FS, "tp"),
            P(FS, None),
            P(FS, None),
            *[P(FS, "tp")] * 6,
        ),
        out_specs=(*[P(FS, "tp")] * 8, P(None, "tp"), P(None, "tp")),
        check_vma=False,
    )
```

```python
import jax
import jax.numpy as jnp
from jax import lax
from jax.experimental import pallas as pl
from jax.experimental.pallas import tpu as pltpu
from jax.sharding import Mesh
from jax.sharding import PartitionSpec as P

D = 4096
QW = 2048
RANK = 256
FS = ("fs_0", "fs_1", "fs_2")
CHIPS = ("fs_0", "fs_1")

beta_one = 0.8
beta_two = 0.9
rate = 0.1

f32 = jnp.float32
bf16 = jnp.bfloat16
f16 = jnp.float16

REACH = 85.0
SHRINK = 2.0**-10

MOMENTS_AT = 128
TOPS_AT = 160
BLOCK_ROWS = 168
GROUP = 8


VMEM = pl.BlockSpec(memory_space=pltpu.VMEM)
SMEM = pl.BlockSpec(memory_space=pltpu.SMEM)


def high_and_low(values):
    high = values.astype(bf16).astype(f32)
    return high, values - high


def pack_kernel(at, qb, ob, qm, om, q1, q2, o1, o2, qc, oc, block, send, cot):
    tp = at[1]
    picked = []
    for basis in (qb, ob):
        full = basis[...].astype(f32)
        part = full[:, :64]
        for t in range(1, 4):
            part = jnp.where(tp == t, full[:, 64 * t : 64 * t + 64], part)
        picked.append(part)
    send[...] = jnp.broadcast_to(jnp.concatenate(picked, axis=1).astype(bf16)[None], send.shape)
    tops = []
    for side, master in ((0, qm), (1, om)):
        values = master[...]
        top = jnp.max(jnp.abs(values), axis=(0, 1), keepdims=True) * 1.01 + 1e-30
        top = top.astype(bf16).astype(f32)
        block[64 * side : 64 * side + 64, :] = jnp.exp(values * (REACH / top)).astype(bf16)
        tops.append(top)
    for side, (first, second) in enumerate(((q1, q2), (o1, o2))):
        first_high, first_low = high_and_low(first[...])
        second_high, second_low = high_and_low(second[...])
        at_row = MOMENTS_AT + 16 * side
        block[at_row : at_row + 16, :] = jnp.concatenate(
            [first_high, second_high, first_low, second_low], axis=0
        ).astype(bf16)
    row = lax.broadcasted_iota(jnp.int32, (8, 512), 0)
    block[TOPS_AT:, :] = jnp.where(row == 0, tops[0], tops[1]).astype(bf16)
    cot[:, :512] = qc[...]
    cot[:, 512:] = oc[...]


def project_kernel(at, saved, layer, mine, theirs, c0, c1, c2, c3, keep, give, saved_near, layer_near, sems):
    copies = [
        pltpu.make_async_copy(saved, saved_near, sems.at[0]),
        pltpu.make_async_copy(layer, layer_near, sems.at[1]),
    ]
    for copy in copies:
        copy.start()
    core = at[0]
    own, other = mine[...], theirs[...]
    first = jnp.where(core == 0, own, other)
    second = jnp.where(core == 0, other, own)
    basis = jnp.concatenate([first, second], axis=1).reshape(D, 128)
    for side, source in ((0, saved_near), (1, layer_near)):
        copies[side].wait()
        coords = jnp.dot(source[...], basis, preferred_element_type=f32)[:, 64 * side : 64 * side + 64]
        high, low = high_and_low(coords.T)
        left = jnp.concatenate([high, low], axis=0).astype(bf16)
        for k, cot in enumerate((c0, c1, c2, c3)):
            both = jnp.dot(left, cot[:, 512 * side : 512 * side + 512], preferred_element_type=f32)
            part = (both[:64] + both[64:]) * SHRINK
            lower, upper = part[:32], part[32:]
            kept = jnp.where(core == 0, lower, upper)
            given = jnp.where(core == 0, upper, lower)
            for j in range(4):
                slot = (side * 4 + k) * 4 + j
                keep[:, slot, :] = kept[:, 128 * j : 128 * j + 128]
                give[:, slot, :] = given[:, 128 * j : 128 * j + 128]


def spread_kernel(at, row, out):
    tp = at[1]
    values = row[...] * (1.0 / SHRINK)
    squares = jnp.broadcast_to(jnp.sum(values * values, axis=(0, 1), keepdims=True), (1, 128))
    for t in range(4):
        k = (tp + 4 - t) % 4
        pieces = []
        for side in range(2):
            for j in range(4):
                pieces.append(row[pl.ds((side * 4 + k) * 4 + j, 1), :] * (1.0 / SHRINK))
        line = jnp.concatenate(pieces + [squares], axis=1)

        def put(chip, carry):
            out[chip * 4 + t] = line
            return carry

        lax.fori_loop(0, 32, put, 0, unroll=True)


def update_kernel(at, mine, theirs, q1, q2, o1, o2, low, factor, qf, qs, of, os):
    core, fs = at[0], at[2]
    total = jnp.sum(mine[:, :, 1024:], axis=0) + jnp.sum(theirs[:, :, 1024:], axis=0)
    scale = lax.rsqrt(1.0 + total * (1.0 / (2.0 * RANK * QW)))
    factor[...] = jnp.broadcast_to(scale, (8, 128))
    is_first = core == 0
    for t in range(4):
        for chip in range(32):
            own, other = mine[chip * 4 + t, :, :1024], theirs[chip * 4 + t, :, :1024]
            low[64 * t + chip : 64 * t + chip + 1, :] = jnp.where(is_first, own, other)
            low[64 * t + 32 + chip : 64 * t + 33 + chip, :] = jnp.where(is_first, other, own)
    near = low[pl.ds(pl.multiple_of(fs // 2 * 8, 8), 8), :]
    own_rows = jnp.where(fs % 2 == 0, near[:4], near[4:]) * scale[:, :1]
    for side, first, second, first_new, second_new in ((0, q1, q2, qf, qs), (1, o1, o2, of, os)):
        scaled = own_rows[:, 512 * side : 512 * side + 512]
        first_new[...] = beta_one * first[...] + (1.0 - beta_one) * scaled
        second_new[...] = beta_two * second[...] + (1.0 - beta_two) * scaled * scaled


def finish_kernel(
    at, factor, low, qb, ob, qm, om, moments, block, tops, *rest
):
    quarters, (qw, ow, qs, os, qc, oc, natural, direction) = rest[:8], rest[8:]
    core, tp = at[0], at[1]

    @pl.when(pl.program_id(0) == 0)
    def _():
        scale = factor[0:1, 0:1]

        def rows(i, carry):
            held = moments[pl.ds(4 * i, 4)].astype(f32)
            lows = low[pl.ds(16 * i, 16), :] * scale
            for side in range(2):
                sums = [held[j, 16 * side : 16 * side + 8] + held[j, 16 * side + 8 : 16 * side + 16] for j in range(4)]
                first = jnp.concatenate([s[:4] for s in sums], axis=0)
                second = jnp.concatenate([s[4:] for s in sums], axis=0)
                scaled = lows[:, 512 * side : 512 * side + 512]
                first = beta_one * first + (1.0 - beta_one) * scaled
                second = beta_two * second + (1.0 - beta_two) * scaled * scaled
                natural[pl.ds(16 * i, 16), 512 * side : 512 * side + 512] = (first / jnp.sqrt(second)).astype(bf16)
            return carry

        lax.fori_loop(0, 16, rows, 0)
        for k in range(4):
            start = pl.multiple_of((tp + 4 - k) % 4 * 64, 64)
            direction[64 * k : 64 * k + 64, :] = natural[pl.ds(start, 64), :]
        for side, basis, master, weight, step in ((0, qb, qm, qw, qs), (1, ob, om, ow, os)):
            moved = jnp.dot(basis[...], natural[:, 512 * side : 512 * side + 512], preferred_element_type=f32)
            step[...] = moved
            weight[...] = master[...] - rate * moved

    bases = []
    for k in range(4):
        own, other = quarters[2 * k][...], quarters[2 * k + 1][...]
        first = jnp.where(core == 0, own, other)
        second = jnp.where(core == 0, other, own)
        bases.append(jnp.concatenate([first, second], axis=1).reshape(GROUP * 64, 128))
    for side, copy in ((0, qc), (1, oc)):
        basis = jnp.concatenate([b[:, 64 * side : 64 * side + 64] for b in bases], axis=1)
        moved = jnp.dot(basis, direction[:, 512 * side : 512 * side + 512], preferred_element_type=f32)
        codes = block[:, 64 * side : 64 * side + 64, :].astype(f32)
        unit = tops[:, side : side + 1, :].astype(f32) * (1.0 / REACH)
        master = (jnp.log(codes) * unit).reshape(GROUP * 64, 512)
        copy[...] = (master - rate * moved).astype(bf16)


def near(*arrays):
    return [pltpu.with_memory_space_constraint(a, pltpu.VMEM) for a in arrays]


def far(*arrays):
    return [pltpu.with_memory_space_constraint(a, pltpu.HBM) for a in arrays]


def swapped(values):
    return lax.ppermute(values, "fs_2", [(0, 1), (1, 0)])


def per_device(
    saved_input,
    query_cotangent,
    layer_cotangent,
    mixed_heads,
    query_basis,
    output_basis,
    query_master,
    output_master,
    query_first,
    query_second,
    output_first,
    output_second,
):
    shape = jax.ShapeDtypeStruct
    at = jnp.stack([lax.axis_index("fs_2"), lax.axis_index("tp"), lax.axis_index(FS)]).astype(jnp.int32)
    moments = (query_first, query_second, output_first, output_second)
    block, send, cot = pl.pallas_call(
        pack_kernel,
        in_specs=[SMEM] + [VMEM] * 10,
        out_specs=[VMEM] * 3,
        out_shape=[shape((BLOCK_ROWS, 512), bf16), shape((32, 64, 128), bf16), shape((256, 1024), bf16)],
        compiler_params=pltpu.CompilerParams(vmem_limit_bytes=24 * 2**20),
        name="pack",
    )(
        at,
        *far(query_basis, output_basis, query_master, output_master, *moments),
        *far(query_cotangent, mixed_heads),
    )
    gathered = lax.all_gather(block, FS, axis=0, tiled=False)
    cots = [cot] + [lax.ppermute(cot, "tp", [(i, (i + k) % 4) for i in range(4)]) for k in (2, 1, 3)]
    cots = [cots[i] for i in (0, 2, 1, 3)]
    mine = lax.all_to_all(send, CHIPS, 0, 0, tiled=True)
    theirs = swapped(mine)
    quarters = [mine, theirs]
    for k in range(1, 4):
        quarter = lax.ppermute(mine, "tp", [(i, (i + k) % 4) for i in range(4)])
        quarters += [quarter, swapped(quarter)]
    keep, give = pl.pallas_call(
        project_kernel,
        in_specs=[SMEM] + [pl.BlockSpec(memory_space=pl.ANY)] * 2 + [VMEM] * 6,
        out_specs=[VMEM] * 2,
        scratch_shapes=[pltpu.VMEM((256, D), bf16)] * 2 + [pltpu.SemaphoreType.DMA((2,))],
        out_shape=[pltpu.VMEM((32, 32, 128), f32)] * 2,
        compiler_params=pltpu.CompilerParams(vmem_limit_bytes=20 * 2**20),
        name="project",
    )(at, *far(saved_input, layer_cotangent), *near(mine, theirs, *cots))
    pair = (keep + swapped(give.astype(f16)).astype(f32)).astype(f16)
    arrived = lax.all_to_all(pair, CHIPS, 0, 0, tiled=True)
    row = jnp.sum(arrived.astype(f32), axis=0)
    out = pl.pallas_call(
        spread_kernel,
        in_specs=[SMEM, VMEM],
        out_specs=VMEM,
        out_shape=pltpu.VMEM((128, 1, 1152), f32),
        compiler_params=pltpu.CompilerParams(vmem_limit_bytes=16 * 2**20),
        name="spread",
    )(at, *near(row))
    mine = lax.all_to_all(out, (*CHIPS, "tp"), 0, 0, tiled=True)
    theirs = swapped(mine)
    low, factor, qf, qs, of, osec = pl.pallas_call(
        update_kernel,
        in_specs=[SMEM] + [VMEM] * 6,
        out_specs=[VMEM] * 6,
        out_shape=[shape((RANK, 1024), f32), shape((8, 128), f32)] + [shape((4, 512), f32)] * 4,
        compiler_params=pltpu.CompilerParams(vmem_limit_bytes=16 * 2**20),
        name="update",
    )(at, *near(mine, theirs), *far(*moments))

    def whole(*dims):
        return pl.BlockSpec(dims, lambda i: (0,) * len(dims))

    local = whole(64, 512)
    query_weight, output_weight, query_step, output_step, query_copy, output_copy = pl.pallas_call(
        finish_kernel,
        grid=(64 // GROUP,),
        in_specs=[
            SMEM,
            whole(8, 128),
            whole(RANK, 1024),
            whole(64, 256),
            whole(64, 256),
            local,
            local,
            pl.BlockSpec((64, 32, 512), lambda i: (0, MOMENTS_AT // 32, 0)),
            pl.BlockSpec((GROUP, 128, 512), lambda i: (i, 0, 0)),
            pl.BlockSpec((GROUP, 8, 512), lambda i: (i, TOPS_AT // 8, 0)),
            *[pl.BlockSpec((GROUP // 2, 64, 128), lambda i: (i, 0, 0))] * 8,
        ],
        out_specs=[local] * 4 + [pl.BlockSpec((GROUP * 64, 512), lambda i: (i, 0))] * 2,
        out_shape=[shape((64, 512), f32)] * 4 + [shape((D, 512), bf16)] * 2,
        scratch_shapes=[pltpu.VMEM((RANK, 1024), bf16)] * 2,
        compiler_params=pltpu.CompilerParams(dimension_semantics=("arbitrary",), vmem_limit_bytes=40 * 2**20),
        name="finish",
    )(
        at,
        *near(factor, low),
        *far(query_basis, output_basis, query_master, output_master, gathered, gathered, gathered, *quarters),
    )
    return (
        query_weight,
        output_weight,
        query_step,
        output_step,
        qf,
        qs,
        of,
        osec,
        query_copy,
        output_copy,
    )


def solution(mesh):
    torus = Mesh(mesh.devices.reshape(8, 4, 2, mesh.shape["tp"]), (*FS, "tp"))
    return jax.shard_map(
        per_device,
        mesh=torus,
        in_specs=(
            P(FS, None),
            P(FS, "tp"),
            P(FS, None),
            P(FS, "tp"),
            P(FS, None),
            P(FS, None),
            *[P(FS, "tp")] * 6,
        ),
        out_specs=(*[P(FS, "tp")] * 8, P(None, "tp"), P(None, "tp")),
        check_vma=False,
    )
```

```python
import jax
import jax.numpy as jnp
from jax import lax
from jax.experimental import pallas as pl
from jax.experimental.pallas import tpu as pltpu
from jax.sharding import Mesh
from jax.sharding import PartitionSpec as P

D = 4096
QW = 2048
RANK = 256
FS = ("fs_0", "fs_1", "fs_2")
CHIPS = ("fs_0", "fs_1")

beta_one = 0.8
beta_two = 0.9
rate = 0.1

f32 = jnp.float32
bf16 = jnp.bfloat16
f16 = jnp.float16

REACH = 85.0
SHRINK = 2.0**-10

MOMENTS_AT = 128
TOPS_AT = 160
BLOCK_ROWS = 168
GROUP = 16


VMEM = pl.BlockSpec(memory_space=pltpu.VMEM)
SMEM = pl.BlockSpec(memory_space=pltpu.SMEM)


def high_and_low(values):
    high = values.astype(bf16).astype(f32)
    return high, values - high


def pack_kernel(at, qb, ob, qm, om, q1, q2, o1, o2, qc, oc, block, send, cot):
    tp = at[1]
    picked = []
    for basis in (qb, ob):
        full = basis[...].astype(f32)
        part = full[:, :64]
        for t in range(1, 4):
            part = jnp.where(tp == t, full[:, 64 * t : 64 * t + 64], part)
        picked.append(part)
    send[...] = jnp.broadcast_to(jnp.concatenate(picked, axis=1).astype(bf16)[None], send.shape)
    tops = []
    for side, master in ((0, qm), (1, om)):
        values = master[...]
        top = jnp.max(jnp.abs(values), axis=(0, 1), keepdims=True) * 1.01 + 1e-30
        top = top.astype(bf16).astype(f32)
        block[64 * side : 64 * side + 64, :] = jnp.exp(values * (REACH / top)).astype(bf16)
        tops.append(top)
    for side, (first, second) in enumerate(((q1, q2), (o1, o2))):
        first_high, first_low = high_and_low(first[...])
        second_high, second_low = high_and_low(second[...])
        at_row = MOMENTS_AT + 16 * side
        block[at_row : at_row + 16, :] = jnp.concatenate(
            [first_high, second_high, first_low, second_low], axis=0
        ).astype(bf16)
    row = lax.broadcasted_iota(jnp.int32, (8, 512), 0)
    block[TOPS_AT:, :] = jnp.where(row == 0, tops[0], tops[1]).astype(bf16)
    cot[:, :512] = qc[...]
    cot[:, 512:] = oc[...]


def project_kernel(at, saved, layer, mine, theirs, c0, c1, c2, c3, keep, give, saved_near, layer_near, sems):
    copies = [
        pltpu.make_async_copy(saved, saved_near, sems.at[0]),
        pltpu.make_async_copy(layer, layer_near, sems.at[1]),
    ]
    for copy in copies:
        copy.start()
    core = at[0]
    own, other = mine[...], theirs[...]
    first = jnp.where(core == 0, own, other)
    second = jnp.where(core == 0, other, own)
    basis = jnp.concatenate([first, second], axis=1).reshape(D, 128)
    for side, source in ((0, saved_near), (1, layer_near)):
        copies[side].wait()
        coords = jnp.dot(source[...], basis, preferred_element_type=f32)[:, 64 * side : 64 * side + 64]
        high, low = high_and_low(coords.T)
        left = jnp.concatenate([high, low], axis=0).astype(bf16)
        for k, cot in enumerate((c0, c1, c2, c3)):
            both = jnp.dot(left, cot[:, 512 * side : 512 * side + 512], preferred_element_type=f32)
            part = (both[:64] + both[64:]) * SHRINK
            lower, upper = part[:32], part[32:]
            kept = jnp.where(core == 0, lower, upper)
            given = jnp.where(core == 0, upper, lower)
            for j in range(4):
                slot = (side * 4 + k) * 4 + j
                keep[:, slot, :] = kept[:, 128 * j : 128 * j + 128]
                give[:, slot, :] = given[:, 128 * j : 128 * j + 128]


def spread_kernel(at, row, out):
    tp = at[1]
    values = row[...] * (1.0 / SHRINK)
    squares = jnp.broadcast_to(jnp.sum(values * values, axis=(0, 1), keepdims=True), (1, 128))
    for t in range(4):
        k = (tp + 4 - t) % 4
        pieces = []
        for side in range(2):
            for j in range(4):
                pieces.append(row[pl.ds((side * 4 + k) * 4 + j, 1), :] * (1.0 / SHRINK))
        line = jnp.concatenate(pieces + [squares], axis=1)

        def put(chip, carry):
            out[chip * 4 + t] = line
            return carry

        lax.fori_loop(0, 32, put, 0, unroll=True)


def update_kernel(at, mine, theirs, q1, q2, o1, o2, low, factor, qf, qs, of, os):
    core, fs = at[0], at[2]
    total = jnp.sum(mine[:, :, 1024:], axis=0) + jnp.sum(theirs[:, :, 1024:], axis=0)
    scale = lax.rsqrt(1.0 + total * (1.0 / (2.0 * RANK * QW)))
    factor[...] = jnp.broadcast_to(scale, (8, 128))
    is_first = core == 0
    for t in range(4):
        for chip in range(32):
            own, other = mine[chip * 4 + t, :, :1024], theirs[chip * 4 + t, :, :1024]
            low[64 * t + chip : 64 * t + chip + 1, :] = jnp.where(is_first, own, other)
            low[64 * t + 32 + chip : 64 * t + 33 + chip, :] = jnp.where(is_first, other, own)
    near = low[pl.ds(pl.multiple_of(fs // 2 * 8, 8), 8), :]
    own_rows = jnp.where(fs % 2 == 0, near[:4], near[4:]) * scale[:, :1]
    for side, first, second, first_new, second_new in ((0, q1, q2, qf, qs), (1, o1, o2, of, os)):
        scaled = own_rows[:, 512 * side : 512 * side + 512]
        first_new[...] = beta_one * first[...] + (1.0 - beta_one) * scaled
        second_new[...] = beta_two * second[...] + (1.0 - beta_two) * scaled * scaled


def finish_kernel(
    at, factor, low, qb, ob, qm, om, moments, block, tops, *rest
):
    quarters, (qw, ow, qs, os, qc, oc, natural, direction) = rest[:8], rest[8:]
    core, tp = at[0], at[1]

    @pl.when(pl.program_id(0) == 0)
    def _():
        scale = factor[0:1, 0:1]

        def rows(i, carry):
            held = moments[pl.ds(4 * i, 4)].astype(f32)
            lows = low[pl.ds(16 * i, 16), :] * scale
            for side in range(2):
                sums = [held[j, 16 * side : 16 * side + 8] + held[j, 16 * side + 8 : 16 * side + 16] for j in range(4)]
                first = jnp.concatenate([s[:4] for s in sums], axis=0)
                second = jnp.concatenate([s[4:] for s in sums], axis=0)
                scaled = lows[:, 512 * side : 512 * side + 512]
                first = beta_one * first + (1.0 - beta_one) * scaled
                second = beta_two * second + (1.0 - beta_two) * scaled * scaled
                natural[pl.ds(16 * i, 16), 512 * side : 512 * side + 512] = (first / jnp.sqrt(second)).astype(bf16)
            return carry

        lax.fori_loop(0, 16, rows, 0)
        for k in range(4):
            start = pl.multiple_of((tp + 4 - k) % 4 * 64, 64)
            direction[64 * k : 64 * k + 64, :] = natural[pl.ds(start, 64), :]
        for side, basis, master, weight, step in ((0, qb, qm, qw, qs), (1, ob, om, ow, os)):
            moved = jnp.dot(basis[...], natural[:, 512 * side : 512 * side + 512], preferred_element_type=f32)
            step[...] = moved
            weight[...] = master[...] - rate * moved

    bases = []
    for k in range(4):
        chips = pl.ds(pl.program_id(0) * (GROUP // 2), GROUP // 2)
        own, other = quarters[k][...], quarters[4][...] if k == 0 else quarters[4 + k][chips]
        first = jnp.where(core == 0, own, other)
        second = jnp.where(core == 0, other, own)
        bases.append(jnp.concatenate([first, second], axis=1).reshape(GROUP * 64, 128))
    for side, copy in ((0, qc), (1, oc)):
        basis = jnp.concatenate([b[:, 64 * side : 64 * side + 64] for b in bases], axis=1)
        moved = jnp.dot(basis, direction[:, 512 * side : 512 * side + 512], preferred_element_type=f32)
        codes = block[:, 64 * side : 64 * side + 64, :].astype(f32)
        unit = tops[:, side : side + 1, :].astype(f32) * (1.0 / REACH)
        master = (jnp.log(codes) * unit).reshape(GROUP * 64, 512)
        copy[...] = (master - rate * moved).astype(bf16)


def near(*arrays):
    return [pltpu.with_memory_space_constraint(a, pltpu.VMEM) for a in arrays]


def far(*arrays):
    return [pltpu.with_memory_space_constraint(a, pltpu.HBM) for a in arrays]


def swapped(values):
    return lax.ppermute(values, "fs_2", [(0, 1), (1, 0)])


def finished(at, factor, low, query_basis, output_basis, query_master, output_master, gathered, quarters):
    shape = jax.ShapeDtypeStruct

    def whole(*dims):
        return pl.BlockSpec(dims, lambda i: (0,) * len(dims))

    local = whole(64, 512)
    return pl.pallas_call(
        finish_kernel,
        grid=(64 // GROUP,),
        in_specs=[
            SMEM,
            whole(8, 128),
            whole(RANK, 1024),
            whole(64, 256),
            whole(64, 256),
            local,
            local,
            pl.BlockSpec((64, 32, 512), lambda i: (0, MOMENTS_AT // 32, 0)),
            pl.BlockSpec((GROUP, 128, 512), lambda i: (i, 0, 0)),
            pl.BlockSpec((GROUP, 8, 512), lambda i: (i, TOPS_AT // 8, 0)),
            *[pl.BlockSpec((GROUP // 2, 64, 128), lambda i: (i, 0, 0))] * 5,
            *[VMEM] * 3,
        ],
        out_specs=[local] * 4 + [pl.BlockSpec((GROUP * 64, 512), lambda i: (i, 0))] * 2,
        out_shape=[shape((64, 512), f32)] * 4 + [shape((D, 512), bf16)] * 2,
        scratch_shapes=[pltpu.VMEM((RANK, 1024), bf16)] * 2,
        compiler_params=pltpu.CompilerParams(dimension_semantics=("arbitrary",), vmem_limit_bytes=40 * 2**20),
        name="finish",
    )(
        at,
        *near(factor, low),
        *far(query_basis, output_basis, query_master, output_master, gathered, gathered, gathered),
        *far(*quarters[:5]),
        *near(*quarters[5:]),
    )


def per_device(
    saved_input,
    query_cotangent,
    layer_cotangent,
    mixed_heads,
    query_basis,
    output_basis,
    query_master,
    output_master,
    query_first,
    query_second,
    output_first,
    output_second,
):
    shape = jax.ShapeDtypeStruct
    at = jnp.stack([lax.axis_index("fs_2"), lax.axis_index("tp"), lax.axis_index(FS)]).astype(jnp.int32)
    moments = (query_first, query_second, output_first, output_second)
    block, send, cot = pl.pallas_call(
        pack_kernel,
        in_specs=[SMEM] + [VMEM] * 10,
        out_specs=[VMEM] * 3,
        out_shape=[shape((BLOCK_ROWS, 512), bf16), shape((32, 64, 128), bf16), shape((256, 1024), bf16)],
        compiler_params=pltpu.CompilerParams(vmem_limit_bytes=24 * 2**20),
        name="pack",
    )(
        at,
        *far(query_basis, output_basis, query_master, output_master, *moments),
        *far(query_cotangent, mixed_heads),
    )
    gathered = lax.all_gather(block, FS, axis=0, tiled=False)
    cots = [cot] + [lax.ppermute(cot, "tp", [(i, (i + k) % 4) for i in range(4)]) for k in (2, 1, 3)]
    cots = [cots[i] for i in (0, 2, 1, 3)]
    mine = lax.all_to_all(send, CHIPS, 0, 0, tiled=True)
    theirs = swapped(mine)
    owns, others = [mine], [theirs]
    for k in range(1, 4):
        quarter = lax.ppermute(mine, "tp", [(i, (i + k) % 4) for i in range(4)])
        owns.append(quarter)
        others.append(swapped(quarter))
    quarters = owns + others
    keep, give = pl.pallas_call(
        project_kernel,
        in_specs=[SMEM] + [pl.BlockSpec(memory_space=pl.ANY)] * 2 + [VMEM] * 6,
        out_specs=[VMEM] * 2,
        scratch_shapes=[pltpu.VMEM((256, D), bf16)] * 2 + [pltpu.SemaphoreType.DMA((2,))],
        out_shape=[pltpu.VMEM((32, 32, 128), f32)] * 2,
        compiler_params=pltpu.CompilerParams(vmem_limit_bytes=20 * 2**20),
        name="project",
    )(at, *far(saved_input, layer_cotangent), *near(mine, theirs, *cots))
    pair = (keep + swapped(give.astype(f16)).astype(f32)).astype(f16)
    arrived = lax.all_to_all(pair, CHIPS, 0, 0, tiled=True)
    row = jnp.sum(arrived.astype(f32), axis=0)
    out = pl.pallas_call(
        spread_kernel,
        in_specs=[SMEM, VMEM],
        out_specs=VMEM,
        out_shape=pltpu.VMEM((128, 1, 1152), f32),
        compiler_params=pltpu.CompilerParams(vmem_limit_bytes=16 * 2**20),
        name="spread",
    )(at, *near(row))
    mine = lax.all_to_all(out, (*CHIPS, "tp"), 0, 0, tiled=True)
    theirs = swapped(mine)
    low, factor, qf, qs, of, osec = pl.pallas_call(
        update_kernel,
        in_specs=[SMEM] + [VMEM] * 6,
        out_specs=[VMEM] * 6,
        out_shape=[shape((RANK, 1024), f32), shape((8, 128), f32)] + [shape((4, 512), f32)] * 4,
        compiler_params=pltpu.CompilerParams(vmem_limit_bytes=16 * 2**20),
        name="update",
    )(at, *near(mine, theirs), *far(*moments))

    query_weight, output_weight, query_step, output_step, query_copy, output_copy = finished(
        at, factor, low, query_basis, output_basis, query_master, output_master, gathered, quarters
    )
    return (
        query_weight,
        output_weight,
        query_step,
        output_step,
        qf,
        qs,
        of,
        osec,
        query_copy,
        output_copy,
    )


def solution(mesh):
    torus = Mesh(mesh.devices.reshape(8, 4, 2, mesh.shape["tp"]), (*FS, "tp"))
    return jax.shard_map(
        per_device,
        mesh=torus,
        in_specs=(
            P(FS, None),
            P(FS, "tp"),
            P(FS, None),
            P(FS, "tp"),
            P(FS, None),
            P(FS, None),
            *[P(FS, "tp")] * 6,
        ),
        out_specs=(*[P(FS, "tp")] * 8, P(None, "tp"), P(None, "tp")),
        check_vma=False,
    )
```

```python
import jax
import jax.numpy as jnp
from jax import lax
from jax.experimental import pallas as pl
from jax.experimental.pallas import tpu as pltpu
from jax.sharding import Mesh
from jax.sharding import PartitionSpec as P

D = 4096
QW = 2048
RANK = 256
FS = ("fs_0", "fs_1", "fs_2")
CHIPS = ("fs_0", "fs_1")

beta_one = 0.8
beta_two = 0.9
rate = 0.1

f32 = jnp.float32
bf16 = jnp.bfloat16
f16 = jnp.float16

REACH = 85.0
SHRINK = 2.0**-10

MOMENTS_AT = 128
TOPS_AT = 144
BLOCK_ROWS = 152
GROUP = 16


VMEM = pl.BlockSpec(memory_space=pltpu.VMEM)
SMEM = pl.BlockSpec(memory_space=pltpu.SMEM)


def high_and_low(values):
    high = values.astype(bf16).astype(f32)
    return high, values - high


def coded(values):
    top = jnp.max(jnp.abs(values), axis=(0, 1), keepdims=True) * 1.01 + 1e-30
    top = top.astype(bf16).astype(f32)
    return jnp.exp(values * (REACH / top)), top


def pack_kernel(at, qb, ob, qm, om, q1, q2, o1, o2, qc, oc, block, send, cot):
    tp = at[1]
    picked = []
    for basis in (qb, ob):
        full = basis[...].astype(f32)
        part = full[:, :64]
        for t in range(1, 4):
            part = jnp.where(tp == t, full[:, 64 * t : 64 * t + 64], part)
        picked.append(part)
    send[...] = jnp.broadcast_to(jnp.concatenate(picked, axis=1).astype(bf16)[None], send.shape)
    row = lax.broadcasted_iota(jnp.int32, (8, 512), 0)
    tops = jnp.zeros((8, 512), f32)
    for side, master in ((0, qm), (1, om)):
        codes, top = coded(master[...])
        block[64 * side : 64 * side + 64, :] = codes.astype(bf16)
        tops = jnp.where(row == side, top, tops)
    held = []
    for side, first, second in ((0, q1, q2), (1, o1, o2)):
        for at_row, values in ((2 + side, first), (4 + side, second)):
            codes, top = coded(values[...])
            held.append(codes)
            tops = jnp.where(row == at_row, top, tops)
    block[MOMENTS_AT : MOMENTS_AT + 16, :] = jnp.concatenate(held, axis=0).astype(bf16)
    block[TOPS_AT:, :] = tops.astype(bf16)
    cot[:, :512] = qc[...]
    cot[:, 512:] = oc[...]


def project_kernel(at, saved, layer, mine, theirs, c0, c1, c2, c3, keep, give, saved_near, layer_near, sems):
    copies = [
        pltpu.make_async_copy(saved, saved_near, sems.at[0]),
        pltpu.make_async_copy(layer, layer_near, sems.at[1]),
    ]
    for copy in copies:
        copy.start()
    core = at[0]
    own, other = mine[...], theirs[...]
    first = jnp.where(core == 0, own, other)
    second = jnp.where(core == 0, other, own)
    basis = jnp.concatenate([first, second], axis=1).reshape(D, 128)
    for side, source in ((0, saved_near), (1, layer_near)):
        copies[side].wait()
        coords = jnp.dot(source[...], basis, preferred_element_type=f32)[:, 64 * side : 64 * side + 64]
        high, low = high_and_low(coords.T)
        left = jnp.concatenate([high, low], axis=0).astype(bf16)
        for k, cot in enumerate((c0, c1, c2, c3)):
            both = jnp.dot(left, cot[:, 512 * side : 512 * side + 512], preferred_element_type=f32)
            part = (both[:64] + both[64:]) * SHRINK
            lower, upper = part[:32], part[32:]
            kept = jnp.where(core == 0, lower, upper)
            given = jnp.where(core == 0, upper, lower)
            for j in range(4):
                slot = (side * 4 + k) * 4 + j
                keep[:, slot, :] = kept[:, 128 * j : 128 * j + 128]
                give[:, slot, :] = given[:, 128 * j : 128 * j + 128]


def spread_kernel(at, row, out):
    tp = at[1]
    values = row[...] * (1.0 / SHRINK)
    squares = jnp.broadcast_to(jnp.sum(values * values, axis=(0, 1), keepdims=True), (1, 128))
    for t in range(4):
        k = (tp + 4 - t) % 4
        pieces = []
        for side in range(2):
            for j in range(4):
                pieces.append(row[pl.ds((side * 4 + k) * 4 + j, 1), :] * (1.0 / SHRINK))
        line = jnp.concatenate(pieces + [squares], axis=1)

        def put(chip, carry):
            out[chip * 4 + t] = line
            return carry

        lax.fori_loop(0, 32, put, 0, unroll=True)


def update_kernel(at, mine, theirs, q1, q2, o1, o2, low, factor, qf, qs, of, os):
    core, fs = at[0], at[2]
    total = jnp.sum(mine[:, :, 1024:], axis=0) + jnp.sum(theirs[:, :, 1024:], axis=0)
    scale = lax.rsqrt(1.0 + total * (1.0 / (2.0 * RANK * QW)))
    factor[...] = jnp.broadcast_to(scale, (8, 128))
    is_first = core == 0
    for t in range(4):
        for chip in range(32):
            own, other = mine[chip * 4 + t, :, :1024], theirs[chip * 4 + t, :, :1024]
            low[64 * t + chip : 64 * t + chip + 1, :] = jnp.where(is_first, own, other)
            low[64 * t + 32 + chip : 64 * t + 33 + chip, :] = jnp.where(is_first, other, own)
    near = low[pl.ds(pl.multiple_of(fs // 2 * 8, 8), 8), :]
    own_rows = jnp.where(fs % 2 == 0, near[:4], near[4:]) * scale[:, :1]
    for side, first, second, first_new, second_new in ((0, q1, q2, qf, qs), (1, o1, o2, of, os)):
        scaled = own_rows[:, 512 * side : 512 * side + 512]
        first_new[...] = beta_one * first[...] + (1.0 - beta_one) * scaled
        second_new[...] = beta_two * second[...] + (1.0 - beta_two) * scaled * scaled


def finish_kernel(
    at, factor, low, qb, ob, qm, om, moments, block, tops, *rest
):
    quarters, (qw, ow, qs, os, qc, oc, natural, direction) = rest[:8], rest[8:]
    core, tp = at[0], at[1]

    @pl.when(pl.program_id(0) == 0)
    def _():
        scale = factor[0:1, 0:1]

        is_first = lax.broadcasted_iota(jnp.int32, (8, 512), 0) < 4

        def rows(i, carry):
            codes = moments[pl.ds(4 * i, 4)].astype(f32)
            units = tops[pl.ds(4 * i, 4)].astype(f32) * (1.0 / REACH)
            lows = low[pl.ds(16 * i, 16), :] * scale
            for side in range(2):
                held = []
                for j in range(4):
                    unit = jnp.where(is_first, units[j, 2 + side : 3 + side], units[j, 4 + side : 5 + side])
                    held.append(jnp.log(codes[j, 8 * side : 8 * side + 8]) * unit)
                first = jnp.concatenate([h[:4] for h in held], axis=0)
                second = jnp.concatenate([h[4:] for h in held], axis=0)
                scaled = lows[:, 512 * side : 512 * side + 512]
                first = beta_one * first + (1.0 - beta_one) * scaled
                second = beta_two * second + (1.0 - beta_two) * scaled * scaled
                natural[pl.ds(16 * i, 16), 512 * side : 512 * side + 512] = (first / jnp.sqrt(second)).astype(bf16)
            return carry

        lax.fori_loop(0, 16, rows, 0)
        for k in range(4):
            start = pl.multiple_of((tp + 4 - k) % 4 * 64, 64)
            direction[64 * k : 64 * k + 64, :] = natural[pl.ds(start, 64), :]
        for side, basis, master, weight, step in ((0, qb, qm, qw, qs), (1, ob, om, ow, os)):
            moved = jnp.dot(basis[...], natural[:, 512 * side : 512 * side + 512], preferred_element_type=f32)
            step[...] = moved
            weight[...] = master[...] - rate * moved

    bases = []
    for k in range(4):
        chips = pl.ds(pl.program_id(0) * (GROUP // 2), GROUP // 2)
        own, other = quarters[k][...], quarters[4][...] if k == 0 else quarters[4 + k][chips]
        first = jnp.where(core == 0, own, other)
        second = jnp.where(core == 0, other, own)
        bases.append(jnp.concatenate([first, second], axis=1).reshape(GROUP * 64, 128))
    for side, copy in ((0, qc), (1, oc)):
        basis = jnp.concatenate([b[:, 64 * side : 64 * side + 64] for b in bases], axis=1)
        moved = jnp.dot(basis, direction[:, 512 * side : 512 * side + 512], preferred_element_type=f32)
        codes = block[:, 64 * side : 64 * side + 64, :].astype(f32)
        blocks = pl.ds(pl.program_id(0) * GROUP, GROUP)
        unit = tops[blocks, side : side + 1, :].astype(f32) * (1.0 / REACH)
        master = (jnp.log(codes) * unit).reshape(GROUP * 64, 512)
        copy[...] = (master - rate * moved).astype(bf16)


def near(*arrays):
    return [pltpu.with_memory_space_constraint(a, pltpu.VMEM) for a in arrays]


def far(*arrays):
    return [pltpu.with_memory_space_constraint(a, pltpu.HBM) for a in arrays]


def swapped(values):
    return lax.ppermute(values, "fs_2", [(0, 1), (1, 0)])


def finished(at, factor, low, query_basis, output_basis, query_master, output_master, gathered, quarters):
    shape = jax.ShapeDtypeStruct

    def whole(*dims):
        return pl.BlockSpec(dims, lambda i: (0,) * len(dims))

    local = whole(64, 512)
    return pl.pallas_call(
        finish_kernel,
        grid=(64 // GROUP,),
        in_specs=[
            SMEM,
            whole(8, 128),
            whole(RANK, 1024),
            whole(64, 256),
            whole(64, 256),
            local,
            local,
            pl.BlockSpec((64, 16, 512), lambda i: (0, MOMENTS_AT // 16, 0)),
            pl.BlockSpec((GROUP, 128, 512), lambda i: (i, 0, 0)),
            pl.BlockSpec((64, 8, 512), lambda i: (0, TOPS_AT // 8, 0)),
            *[pl.BlockSpec((GROUP // 2, 64, 128), lambda i: (i, 0, 0))] * 5,
            *[VMEM] * 3,
        ],
        out_specs=[local] * 4 + [pl.BlockSpec((GROUP * 64, 512), lambda i: (i, 0))] * 2,
        out_shape=[shape((64, 512), f32)] * 4 + [shape((D, 512), bf16)] * 2,
        scratch_shapes=[pltpu.VMEM((RANK, 1024), bf16)] * 2,
        compiler_params=pltpu.CompilerParams(dimension_semantics=("arbitrary",), vmem_limit_bytes=40 * 2**20),
        name="finish",
    )(
        at,
        *near(factor, low),
        *far(query_basis, output_basis, query_master, output_master, gathered, gathered, gathered),
        *far(*quarters[:5]),
        *near(*quarters[5:]),
    )


def per_device(
    saved_input,
    query_cotangent,
    layer_cotangent,
    mixed_heads,
    query_basis,
    output_basis,
    query_master,
    output_master,
    query_first,
    query_second,
    output_first,
    output_second,
):
    shape = jax.ShapeDtypeStruct
    at = jnp.stack([lax.axis_index("fs_2"), lax.axis_index("tp"), lax.axis_index(FS)]).astype(jnp.int32)
    moments = (query_first, query_second, output_first, output_second)
    block, send, cot = pl.pallas_call(
        pack_kernel,
        in_specs=[SMEM] + [VMEM] * 10,
        out_specs=[VMEM] * 3,
        out_shape=[shape((BLOCK_ROWS, 512), bf16), shape((32, 64, 128), bf16), shape((256, 1024), bf16)],
        compiler_params=pltpu.CompilerParams(vmem_limit_bytes=24 * 2**20),
        name="pack",
    )(
        at,
        *far(query_basis, output_basis, query_master, output_master, *moments),
        *far(query_cotangent, mixed_heads),
    )
    gathered = lax.all_gather(block, FS, axis=0, tiled=False)
    cots = [cot] + [lax.ppermute(cot, "tp", [(i, (i + k) % 4) for i in range(4)]) for k in (2, 1, 3)]
    cots = [cots[i] for i in (0, 2, 1, 3)]
    mine = lax.all_to_all(send, CHIPS, 0, 0, tiled=True)
    theirs = swapped(mine)
    owns, others = [mine], [theirs]
    for k in range(1, 4):
        quarter = lax.ppermute(mine, "tp", [(i, (i + k) % 4) for i in range(4)])
        owns.append(quarter)
        others.append(swapped(quarter))
    quarters = owns + others
    keep, give = pl.pallas_call(
        project_kernel,
        in_specs=[SMEM] + [pl.BlockSpec(memory_space=pl.ANY)] * 2 + [VMEM] * 6,
        out_specs=[VMEM] * 2,
        scratch_shapes=[pltpu.VMEM((256, D), bf16)] * 2 + [pltpu.SemaphoreType.DMA((2,))],
        out_shape=[pltpu.VMEM((32, 32, 128), f32)] * 2,
        compiler_params=pltpu.CompilerParams(vmem_limit_bytes=20 * 2**20),
        name="project",
    )(at, *far(saved_input, layer_cotangent), *near(mine, theirs, *cots))
    pair = (keep + swapped(give.astype(f16)).astype(f32)).astype(f16)
    arrived = lax.all_to_all(pair, CHIPS, 0, 0, tiled=True)
    row = jnp.sum(arrived.astype(f32), axis=0)
    out = pl.pallas_call(
        spread_kernel,
        in_specs=[SMEM, VMEM],
        out_specs=VMEM,
        out_shape=pltpu.VMEM((128, 1, 1152), f32),
        compiler_params=pltpu.CompilerParams(vmem_limit_bytes=16 * 2**20),
        name="spread",
    )(at, *near(row))
    mine = lax.all_to_all(out, (*CHIPS, "tp"), 0, 0, tiled=True)
    theirs = swapped(mine)
    low, factor, qf, qs, of, osec = pl.pallas_call(
        update_kernel,
        in_specs=[SMEM] + [VMEM] * 6,
        out_specs=[VMEM] * 6,
        out_shape=[shape((RANK, 1024), f32), shape((8, 128), f32)] + [shape((4, 512), f32)] * 4,
        compiler_params=pltpu.CompilerParams(vmem_limit_bytes=16 * 2**20),
        name="update",
    )(at, *near(mine, theirs), *far(*moments))

    query_weight, output_weight, query_step, output_step, query_copy, output_copy = finished(
        at, factor, low, query_basis, output_basis, query_master, output_master, gathered, quarters
    )
    return (
        query_weight,
        output_weight,
        query_step,
        output_step,
        qf,
        qs,
        of,
        osec,
        query_copy,
        output_copy,
    )


def solution(mesh):
    torus = Mesh(mesh.devices.reshape(8, 4, 2, mesh.shape["tp"]), (*FS, "tp"))
    return jax.shard_map(
        per_device,
        mesh=torus,
        in_specs=(
            P(FS, None),
            P(FS, "tp"),
            P(FS, None),
            P(FS, "tp"),
            P(FS, None),
            P(FS, None),
            *[P(FS, "tp")] * 6,
        ),
        out_specs=(*[P(FS, "tp")] * 8, P(None, "tp"), P(None, "tp")),
        check_vma=False,
    )
```

```python
import jax
import jax.numpy as jnp
from jax import lax
from jax.experimental import pallas as pl
from jax.experimental.pallas import tpu as pltpu
from jax.sharding import Mesh
from jax.sharding import PartitionSpec as P

D = 4096
QW = 2048
RANK = 256
FS = ("fs_0", "fs_1", "fs_2")
CHIPS = ("fs_0", "fs_1")

beta_one = 0.8
beta_two = 0.9
rate = 0.1

f32 = jnp.float32
bf16 = jnp.bfloat16
f16 = jnp.float16

REACH = 85.0
SHRINK = 2.0**-10

MOMENTS_AT = 128
TOPS_AT = 144
BLOCK_ROWS = 152
GROUP = 16


VMEM = pl.BlockSpec(memory_space=pltpu.VMEM)
SMEM = pl.BlockSpec(memory_space=pltpu.SMEM)


def high_and_low(values):
    high = values.astype(bf16).astype(f32)
    return high, values - high


def coded(values):
    top = jnp.max(jnp.abs(values), axis=(0, 1), keepdims=True) * 1.01 + 1e-30
    top = top.astype(bf16).astype(f32)
    return jnp.exp(values * (REACH / top)), top


def pack_kernel(at, qb, ob, qm, om, q1, q2, o1, o2, qc, oc, saved, block, send, cot, saved_near, sem):
    staged = pltpu.make_async_copy(saved, saved_near, sem)
    staged.start()
    tp = at[1]
    picked = []
    for basis in (qb, ob):
        full = basis[...].astype(f32)
        part = full[:, :64]
        for t in range(1, 4):
            part = jnp.where(tp == t, full[:, 64 * t : 64 * t + 64], part)
        picked.append(part)
    send[...] = jnp.broadcast_to(jnp.concatenate(picked, axis=1).astype(bf16)[None], send.shape)
    row = lax.broadcasted_iota(jnp.int32, (8, 512), 0)
    tops = jnp.zeros((8, 512), f32)
    for side, master in ((0, qm), (1, om)):
        codes, top = coded(master[...])
        block[64 * side : 64 * side + 64, :] = codes.astype(bf16)
        tops = jnp.where(row == side, top, tops)
    held = []
    for side, first, second in ((0, q1, q2), (1, o1, o2)):
        for at_row, values in ((2 + side, first), (4 + side, second)):
            codes, top = coded(values[...])
            held.append(codes)
            tops = jnp.where(row == at_row, top, tops)
    block[MOMENTS_AT : MOMENTS_AT + 16, :] = jnp.concatenate(held, axis=0).astype(bf16)
    block[TOPS_AT:, :] = tops.astype(bf16)
    cot[:, :512] = qc[...]
    cot[:, 512:] = oc[...]
    staged.wait()


def project_kernel(at, saved, layer, mine, theirs, c0, c1, c2, c3, keep, give, layer_near, sem):
    staged = pltpu.make_async_copy(layer, layer_near, sem)
    staged.start()
    core = at[0]
    own, other = mine[...], theirs[...]
    first = jnp.where(core == 0, own, other)
    second = jnp.where(core == 0, other, own)
    basis = jnp.concatenate([first, second], axis=1).reshape(D, 128)
    for side, source in ((0, saved), (1, layer_near)):
        if side == 1:
            staged.wait()
        coords = jnp.dot(source[...], basis, preferred_element_type=f32)[:, 64 * side : 64 * side + 64]
        high, low = high_and_low(coords.T)
        left = jnp.concatenate([high, low], axis=0).astype(bf16)
        for k, cot in enumerate((c0, c1, c2, c3)):
            both = jnp.dot(left, cot[:, 512 * side : 512 * side + 512], preferred_element_type=f32)
            part = (both[:64] + both[64:]) * SHRINK
            lower, upper = part[:32], part[32:]
            kept = jnp.where(core == 0, lower, upper)
            given = jnp.where(core == 0, upper, lower)
            for j in range(4):
                slot = (side * 4 + k) * 4 + j
                keep[:, slot, :] = kept[:, 128 * j : 128 * j + 128]
                give[:, slot, :] = given[:, 128 * j : 128 * j + 128]


def spread_kernel(at, row, out):
    tp = at[1]
    values = row[...] * (1.0 / SHRINK)
    squares = jnp.broadcast_to(jnp.sum(values * values, axis=(0, 1), keepdims=True), (1, 128))
    for t in range(4):
        k = (tp + 4 - t) % 4
        pieces = []
        for side in range(2):
            for j in range(4):
                pieces.append(row[pl.ds((side * 4 + k) * 4 + j, 1), :] * (1.0 / SHRINK))
        line = jnp.concatenate(pieces + [squares], axis=1)

        def put(chip, carry):
            out[chip * 4 + t] = line
            return carry

        lax.fori_loop(0, 32, put, 0, unroll=True)


def update_kernel(at, mine, theirs, q1, q2, o1, o2, low, factor, qf, qs, of, os):
    core, fs = at[0], at[2]
    total = jnp.sum(mine[:, :, 1024:], axis=0) + jnp.sum(theirs[:, :, 1024:], axis=0)
    scale = lax.rsqrt(1.0 + total * (1.0 / (2.0 * RANK * QW)))
    factor[...] = jnp.broadcast_to(scale, (8, 128))
    is_first = core == 0
    for t in range(4):
        for chip in range(32):
            own, other = mine[chip * 4 + t, :, :1024], theirs[chip * 4 + t, :, :1024]
            low[64 * t + chip : 64 * t + chip + 1, :] = jnp.where(is_first, own, other)
            low[64 * t + 32 + chip : 64 * t + 33 + chip, :] = jnp.where(is_first, other, own)
    near = low[pl.ds(pl.multiple_of(fs // 2 * 8, 8), 8), :]
    own_rows = jnp.where(fs % 2 == 0, near[:4], near[4:]) * scale[:, :1]
    for side, first, second, first_new, second_new in ((0, q1, q2, qf, qs), (1, o1, o2, of, os)):
        scaled = own_rows[:, 512 * side : 512 * side + 512]
        first_new[...] = beta_one * first[...] + (1.0 - beta_one) * scaled
        second_new[...] = beta_two * second[...] + (1.0 - beta_two) * scaled * scaled


def finish_kernel(
    at, factor, low, qb, ob, qm, om, moments, gathered, tops, *rest
):
    quarters, (qw, ow, qs, os, qc, oc, natural, direction, held_codes, sems) = rest[:8], rest[8:]
    core, tp = at[0], at[1]
    step, steps = pl.program_id(0), 64 // GROUP

    def fetch(i):
        source = gathered.at[pl.ds(i * GROUP, GROUP), pl.ds(0, 128), :]
        return pltpu.make_async_copy(source, held_codes.at[i % 2], sems.at[i % 2])

    @pl.when(step == 0)
    def _():
        fetch(0).start()

    @pl.when(step + 1 < steps)
    def _():
        fetch(step + 1).start()

    @pl.when(pl.program_id(0) == 0)
    def _():
        scale = factor[0:1, 0:1]

        is_first = lax.broadcasted_iota(jnp.int32, (8, 512), 0) < 4

        def rows(i, carry):
            codes = moments[pl.ds(4 * i, 4)].astype(f32)
            units = tops[pl.ds(4 * i, 4)].astype(f32) * (1.0 / REACH)
            lows = low[pl.ds(16 * i, 16), :] * scale
            for side in range(2):
                held = []
                for j in range(4):
                    unit = jnp.where(is_first, units[j, 2 + side : 3 + side], units[j, 4 + side : 5 + side])
                    held.append(jnp.log(codes[j, 8 * side : 8 * side + 8]) * unit)
                first = jnp.concatenate([h[:4] for h in held], axis=0)
                second = jnp.concatenate([h[4:] for h in held], axis=0)
                scaled = lows[:, 512 * side : 512 * side + 512]
                first = beta_one * first + (1.0 - beta_one) * scaled
                second = beta_two * second + (1.0 - beta_two) * scaled * scaled
                natural[pl.ds(16 * i, 16), 512 * side : 512 * side + 512] = (first / jnp.sqrt(second)).astype(bf16)
            return carry

        lax.fori_loop(0, 16, rows, 0, unroll=4)
        for k in range(4):
            start = pl.multiple_of((tp + 4 - k) % 4 * 64, 64)
            direction[64 * k : 64 * k + 64, :] = natural[pl.ds(start, 64), :]
        for side, basis, master, weight, step in ((0, qb, qm, qw, qs), (1, ob, om, ow, os)):
            moved = jnp.dot(basis[...], natural[:, 512 * side : 512 * side + 512], preferred_element_type=f32)
            step[...] = moved
            weight[...] = master[...] - rate * moved

    fetch(step).wait()
    block = held_codes.at[step % 2]
    bases = []
    for k in range(4):
        chips = pl.ds(pl.program_id(0) * (GROUP // 2), GROUP // 2)
        own, other = quarters[k][...], quarters[4][...] if k == 0 else quarters[4 + k][chips]
        first = jnp.where(core == 0, own, other)
        second = jnp.where(core == 0, other, own)
        bases.append(jnp.concatenate([first, second], axis=1).reshape(GROUP * 64, 128))
    for side, copy in ((0, qc), (1, oc)):
        basis = jnp.concatenate([b[:, 64 * side : 64 * side + 64] for b in bases], axis=1)
        moved = jnp.dot(basis, direction[:, 512 * side : 512 * side + 512], preferred_element_type=f32)
        codes = block[:, 64 * side : 64 * side + 64, :].astype(f32)
        blocks = pl.ds(pl.program_id(0) * GROUP, GROUP)
        unit = tops[blocks, side : side + 1, :].astype(f32) * (1.0 / REACH)
        master = (jnp.log(codes) * unit).reshape(GROUP * 64, 512)
        copy[...] = (master - rate * moved).astype(bf16)


def near(*arrays):
    return [pltpu.with_memory_space_constraint(a, pltpu.VMEM) for a in arrays]


def far(*arrays):
    return [pltpu.with_memory_space_constraint(a, pltpu.HBM) for a in arrays]


def swapped(values):
    return lax.ppermute(values, "fs_2", [(0, 1), (1, 0)])


def finished(at, factor, low, query_basis, output_basis, query_master, output_master, gathered, quarters):
    shape = jax.ShapeDtypeStruct

    def whole(*dims):
        return pl.BlockSpec(dims, lambda i: (0,) * len(dims))

    local = whole(64, 512)
    return pl.pallas_call(
        finish_kernel,
        grid=(64 // GROUP,),
        in_specs=[
            SMEM,
            whole(8, 128),
            whole(RANK, 1024),
            whole(64, 256),
            whole(64, 256),
            local,
            local,
            pl.BlockSpec((64, 16, 512), lambda i: (0, MOMENTS_AT // 16, 0)),
            pl.BlockSpec(memory_space=pl.ANY),
            pl.BlockSpec((64, 8, 512), lambda i: (0, TOPS_AT // 8, 0)),
            *[pl.BlockSpec((GROUP // 2, 64, 128), lambda i: (i, 0, 0))] * 5,
            *[VMEM] * 3,
        ],
        out_specs=[local] * 4 + [pl.BlockSpec((GROUP * 64, 512), lambda i: (i, 0))] * 2,
        out_shape=[shape((64, 512), f32)] * 4 + [shape((D, 512), bf16)] * 2,
        scratch_shapes=[pltpu.VMEM((RANK, 1024), bf16)] * 2
        + [pltpu.VMEM((2, GROUP, 128, 512), bf16), pltpu.SemaphoreType.DMA((2,))],
        compiler_params=pltpu.CompilerParams(dimension_semantics=("arbitrary",), vmem_limit_bytes=40 * 2**20),
        name="finish",
    )(
        at,
        *near(factor, low),
        *far(query_basis, output_basis, query_master, output_master, gathered, gathered, gathered),
        *far(*quarters[:5]),
        *near(*quarters[5:]),
    )


def per_device(
    saved_input,
    query_cotangent,
    layer_cotangent,
    mixed_heads,
    query_basis,
    output_basis,
    query_master,
    output_master,
    query_first,
    query_second,
    output_first,
    output_second,
):
    shape = jax.ShapeDtypeStruct
    at = jnp.stack([lax.axis_index("fs_2"), lax.axis_index("tp"), lax.axis_index(FS)]).astype(jnp.int32)
    moments = (query_first, query_second, output_first, output_second)
    block, send, cot, saved_near = pl.pallas_call(
        pack_kernel,
        in_specs=[SMEM] + [VMEM] * 10 + [pl.BlockSpec(memory_space=pl.ANY)],
        out_specs=[VMEM] * 4,
        out_shape=[
            shape((BLOCK_ROWS, 512), bf16),
            shape((32, 64, 128), bf16),
            shape((256, 1024), bf16),
            pltpu.VMEM((256, D), bf16),
        ],
        scratch_shapes=[pltpu.SemaphoreType.DMA],
        compiler_params=pltpu.CompilerParams(vmem_limit_bytes=24 * 2**20),
        name="pack",
    )(
        at,
        *far(query_basis, output_basis, query_master, output_master, *moments),
        *far(query_cotangent, mixed_heads, saved_input),
    )
    gathered = lax.all_gather(block, FS, axis=0, tiled=False)
    cots = [cot] + [lax.ppermute(cot, "tp", [(i, (i + k) % 4) for i in range(4)]) for k in (2, 1, 3)]
    cots = [cots[i] for i in (0, 2, 1, 3)]
    mine = lax.all_to_all(send, CHIPS, 0, 0, tiled=True)
    theirs = swapped(mine)
    owns, others = [mine], [theirs]
    for k in range(1, 4):
        quarter = lax.ppermute(mine, "tp", [(i, (i + k) % 4) for i in range(4)])
        owns.append(quarter)
        others.append(swapped(quarter))
    quarters = owns + others
    keep, give = pl.pallas_call(
        project_kernel,
        in_specs=[SMEM, VMEM, pl.BlockSpec(memory_space=pl.ANY)] + [VMEM] * 6,
        out_specs=[VMEM] * 2,
        scratch_shapes=[pltpu.VMEM((256, D), bf16), pltpu.SemaphoreType.DMA],
        out_shape=[pltpu.VMEM((32, 32, 128), f32)] * 2,
        compiler_params=pltpu.CompilerParams(vmem_limit_bytes=20 * 2**20),
        name="project",
    )(at, *near(saved_near), *far(layer_cotangent), *near(mine, theirs, *cots))
    pair = (keep + swapped(give.astype(f16)).astype(f32)).astype(f16)
    arrived = lax.all_to_all(pair, CHIPS, 0, 0, tiled=True)
    row = jnp.sum(arrived.astype(f32), axis=0)
    out = pl.pallas_call(
        spread_kernel,
        in_specs=[SMEM, VMEM],
        out_specs=VMEM,
        out_shape=pltpu.VMEM((128, 1, 1152), f32),
        compiler_params=pltpu.CompilerParams(vmem_limit_bytes=16 * 2**20),
        name="spread",
    )(at, *near(row))
    mine = lax.all_to_all(out, (*CHIPS, "tp"), 0, 0, tiled=True)
    theirs = swapped(mine)
    low, factor, qf, qs, of, osec = pl.pallas_call(
        update_kernel,
        in_specs=[SMEM] + [VMEM] * 6,
        out_specs=[VMEM] * 6,
        out_shape=[shape((RANK, 1024), f32), shape((8, 128), f32)] + [shape((4, 512), f32)] * 4,
        compiler_params=pltpu.CompilerParams(vmem_limit_bytes=16 * 2**20),
        name="update",
    )(at, *near(mine, theirs), *far(*moments))

    query_weight, output_weight, query_step, output_step, query_copy, output_copy = finished(
        at, factor, low, query_basis, output_basis, query_master, output_master, gathered, quarters
    )
    return (
        query_weight,
        output_weight,
        query_step,
        output_step,
        qf,
        qs,
        of,
        osec,
        query_copy,
        output_copy,
    )


def solution(mesh):
    torus = Mesh(mesh.devices.reshape(8, 4, 2, mesh.shape["tp"]), (*FS, "tp"))
    return jax.shard_map(
        per_device,
        mesh=torus,
        in_specs=(
            P(FS, None),
            P(FS, "tp"),
            P(FS, None),
            P(FS, "tp"),
            P(FS, None),
            P(FS, None),
            *[P(FS, "tp")] * 6,
        ),
        out_specs=(*[P(FS, "tp")] * 8, P(None, "tp"), P(None, "tp")),
        check_vma=False,
    )
```

```python
import jax
import jax.numpy as jnp
from jax import lax
from jax.experimental import pallas as pl
from jax.experimental.pallas import tpu as pltpu
from jax.sharding import Mesh
from jax.sharding import PartitionSpec as P

D = 4096
QW = 2048
RANK = 256
FS = ("fs_0", "fs_1", "fs_2")
CHIPS = ("fs_0", "fs_1")

beta_one = 0.8
beta_two = 0.9
rate = 0.1

f32 = jnp.float32
bf16 = jnp.bfloat16
f16 = jnp.float16

REACH = 85.0
SHRINK = 2.0**-10

MOMENTS_AT = 128
TOPS_AT = 144
BLOCK_ROWS = 152
GROUP = 16


VMEM = pl.BlockSpec(memory_space=pltpu.VMEM)
SMEM = pl.BlockSpec(memory_space=pltpu.SMEM)


def high_and_low(values):
    high = values.astype(bf16).astype(f32)
    return high, values - high


def coded(values):
    top = jnp.max(jnp.abs(values), axis=(0, 1), keepdims=True) * 1.01 + 1e-30
    top = top.astype(bf16).astype(f32)
    return jnp.exp(values * (REACH / top)), top


def pack_kernel(at, qb, ob, qm, om, q1, q2, o1, o2, qc, oc, block, send, cot):
    tp = at[1]
    picked = []
    for basis in (qb, ob):
        full = basis[...].astype(f32)
        part = full[:, :64]
        for t in range(1, 4):
            part = jnp.where(tp == t, full[:, 64 * t : 64 * t + 64], part)
        picked.append(part)
    send[...] = jnp.broadcast_to(jnp.concatenate(picked, axis=1).astype(bf16)[None], send.shape)
    row = lax.broadcasted_iota(jnp.int32, (8, 512), 0)
    tops = jnp.zeros((8, 512), f32)
    for side, master in ((0, qm), (1, om)):
        codes, top = coded(master[...])
        block[64 * side : 64 * side + 64, :] = codes.astype(bf16)
        tops = jnp.where(row == side, top, tops)
    held = []
    for side, first, second in ((0, q1, q2), (1, o1, o2)):
        for at_row, values in ((2 + side, first), (4 + side, second)):
            codes, top = coded(values[...])
            held.append(codes)
            tops = jnp.where(row == at_row, top, tops)
    block[MOMENTS_AT : MOMENTS_AT + 16, :] = jnp.concatenate(held, axis=0).astype(bf16)
    block[TOPS_AT:, :] = tops.astype(bf16)
    cot[:, :512] = qc[...]
    cot[:, 512:] = oc[...]


def project_kernel(at, saved, layer, mine, theirs, c0, c1, c2, c3, keep, give, saved_near, layer_near, sems):
    copies = [
        pltpu.make_async_copy(saved, saved_near, sems.at[0]),
        pltpu.make_async_copy(layer, layer_near, sems.at[1]),
    ]
    for copy in copies:
        copy.start()
    core = at[0]
    own, other = mine[...], theirs[...]
    first = jnp.where(core == 0, own, other)
    second = jnp.where(core == 0, other, own)
    basis = jnp.concatenate([first, second], axis=1).reshape(D, 128)
    for side, source in ((0, saved_near), (1, layer_near)):
        copies[side].wait()
        coords = jnp.dot(source[...], basis, preferred_element_type=f32)[:, 64 * side : 64 * side + 64]
        high, low = high_and_low(coords.T)
        left = jnp.concatenate([high, low], axis=0).astype(bf16)
        for k, cot in enumerate((c0, c1, c2, c3)):
            both = jnp.dot(left, cot[:, 512 * side : 512 * side + 512], preferred_element_type=f32)
            part = (both[:64] + both[64:]) * SHRINK
            lower, upper = part[:32], part[32:]
            kept = jnp.where(core == 0, lower, upper)
            given = jnp.where(core == 0, upper, lower)
            for j in range(4):
                slot = (side * 4 + k) * 4 + j
                keep[:, slot, :] = kept[:, 128 * j : 128 * j + 128]
                give[:, slot, :] = given[:, 128 * j : 128 * j + 128]


def spread_kernel(at, row, out):
    tp = at[1]
    values = row[...] * (1.0 / SHRINK)
    squares = jnp.broadcast_to(jnp.sum(values * values, axis=(0, 1), keepdims=True), (1, 128))
    for t in range(4):
        k = (tp + 4 - t) % 4
        pieces = []
        for side in range(2):
            for j in range(4):
                pieces.append(row[pl.ds((side * 4 + k) * 4 + j, 1), :] * (1.0 / SHRINK))
        line = jnp.concatenate(pieces + [squares], axis=1)

        def put(chip, carry):
            out[chip * 4 + t] = line
            return carry

        lax.fori_loop(0, 32, put, 0, unroll=True)


def update_kernel(at, mine, theirs, q1, q2, o1, o2, low, factor, qf, qs, of, os):
    core, fs = at[0], at[2]
    total = jnp.sum(mine[:, :, 1024:], axis=0) + jnp.sum(theirs[:, :, 1024:], axis=0)
    scale = lax.rsqrt(1.0 + total * (1.0 / (2.0 * RANK * QW)))
    factor[...] = jnp.broadcast_to(scale, (8, 128))
    is_first = core == 0
    for t in range(4):
        for chip in range(32):
            own, other = mine[chip * 4 + t, :, :1024], theirs[chip * 4 + t, :, :1024]
            low[64 * t + chip : 64 * t + chip + 1, :] = jnp.where(is_first, own, other)
            low[64 * t + 32 + chip : 64 * t + 33 + chip, :] = jnp.where(is_first, other, own)
    near = low[pl.ds(pl.multiple_of(fs // 2 * 8, 8), 8), :]
    own_rows = jnp.where(fs % 2 == 0, near[:4], near[4:]) * scale[:, :1]
    for side, first, second, first_new, second_new in ((0, q1, q2, qf, qs), (1, o1, o2, of, os)):
        scaled = own_rows[:, 512 * side : 512 * side + 512]
        first_new[...] = beta_one * first[...] + (1.0 - beta_one) * scaled
        second_new[...] = beta_two * second[...] + (1.0 - beta_two) * scaled * scaled


def finish_kernel(
    at, factor, low, qb, ob, qm, om, moments, gathered, tops, *rest
):
    quarters, (qw, ow, qs, os, qc, oc, natural, direction, held_codes, sems) = rest[:8], rest[8:]
    core, tp = at[0], at[1]
    step, steps = pl.program_id(0), 64 // GROUP

    def fetch(i):
        source = gathered.at[pl.ds(i * GROUP, GROUP), pl.ds(0, 128), :]
        return pltpu.make_async_copy(source, held_codes.at[i % 2], sems.at[i % 2])

    @pl.when(step == 0)
    def _():
        fetch(0).start()

    @pl.when(step + 1 < steps)
    def _():
        fetch(step + 1).start()

    @pl.when(pl.program_id(0) == 0)
    def _():
        scale = factor[0:1, 0:1]

        is_first = lax.broadcasted_iota(jnp.int32, (8, 512), 0) < 4

        def rows(i, carry):
            codes = moments[pl.ds(4 * i, 4)].astype(f32)
            units = tops[pl.ds(4 * i, 4)].astype(f32) * (1.0 / REACH)
            lows = low[pl.ds(16 * i, 16), :] * scale
            for side in range(2):
                held = []
                for j in range(4):
                    unit = jnp.where(is_first, units[j, 2 + side : 3 + side], units[j, 4 + side : 5 + side])
                    held.append(jnp.log(codes[j, 8 * side : 8 * side + 8]) * unit)
                first = jnp.concatenate([h[:4] for h in held], axis=0)
                second = jnp.concatenate([h[4:] for h in held], axis=0)
                scaled = lows[:, 512 * side : 512 * side + 512]
                first = beta_one * first + (1.0 - beta_one) * scaled
                second = beta_two * second + (1.0 - beta_two) * scaled * scaled
                natural[pl.ds(16 * i, 16), 512 * side : 512 * side + 512] = (first / jnp.sqrt(second)).astype(bf16)
            return carry

        lax.fori_loop(0, 16, rows, 0, unroll=4)
        for k in range(4):
            start = pl.multiple_of((tp + 4 - k) % 4 * 64, 64)
            direction[64 * k : 64 * k + 64, :] = natural[pl.ds(start, 64), :]
        for side, basis, master, weight, step in ((0, qb, qm, qw, qs), (1, ob, om, ow, os)):
            moved = jnp.dot(basis[...], natural[:, 512 * side : 512 * side + 512], preferred_element_type=f32)
            step[...] = moved
            weight[...] = master[...] - rate * moved

    fetch(step).wait()
    block = held_codes.at[step % 2]
    bases = []
    for k in range(4):
        chips = pl.ds(pl.program_id(0) * (GROUP // 2), GROUP // 2)
        own, other = quarters[k][...], quarters[4][...] if k == 0 else quarters[4 + k][chips]
        first = jnp.where(core == 0, own, other)
        second = jnp.where(core == 0, other, own)
        bases.append(jnp.concatenate([first, second], axis=1).reshape(GROUP * 64, 128))
    for side, copy in ((0, qc), (1, oc)):
        basis = jnp.concatenate([b[:, 64 * side : 64 * side + 64] for b in bases], axis=1)
        moved = jnp.dot(basis, direction[:, 512 * side : 512 * side + 512], preferred_element_type=f32)
        codes = block[:, 64 * side : 64 * side + 64, :].astype(f32)
        blocks = pl.ds(pl.program_id(0) * GROUP, GROUP)
        unit = tops[blocks, side : side + 1, :].astype(f32) * (1.0 / REACH)
        master = (jnp.log(codes) * unit).reshape(GROUP * 64, 512)
        copy[...] = (master - rate * moved).astype(bf16)


def near(*arrays):
    return [pltpu.with_memory_space_constraint(a, pltpu.VMEM) for a in arrays]


def far(*arrays):
    return [pltpu.with_memory_space_constraint(a, pltpu.HBM) for a in arrays]


def swapped(values):
    return lax.ppermute(values, "fs_2", [(0, 1), (1, 0)])


def finished(at, factor, low, query_basis, output_basis, query_master, output_master, gathered, quarters):
    shape = jax.ShapeDtypeStruct

    def whole(*dims):
        return pl.BlockSpec(dims, lambda i: (0,) * len(dims))

    local = whole(64, 512)
    return pl.pallas_call(
        finish_kernel,
        grid=(64 // GROUP,),
        in_specs=[
            SMEM,
            whole(8, 128),
            whole(RANK, 1024),
            whole(64, 256),
            whole(64, 256),
            local,
            local,
            pl.BlockSpec((64, 16, 512), lambda i: (0, MOMENTS_AT // 16, 0)),
            pl.BlockSpec(memory_space=pl.ANY),
            pl.BlockSpec((64, 8, 512), lambda i: (0, TOPS_AT // 8, 0)),
            *[pl.BlockSpec((GROUP // 2, 64, 128), lambda i: (i, 0, 0))] * 5,
            *[VMEM] * 3,
        ],
        out_specs=[local] * 4 + [pl.BlockSpec((GROUP * 64, 512), lambda i: (i, 0))] * 2,
        out_shape=[shape((64, 512), f32)] * 4 + [shape((D, 512), bf16)] * 2,
        scratch_shapes=[pltpu.VMEM((RANK, 1024), bf16)] * 2
        + [pltpu.VMEM((2, GROUP, 128, 512), bf16), pltpu.SemaphoreType.DMA((2,))],
        compiler_params=pltpu.CompilerParams(dimension_semantics=("arbitrary",), vmem_limit_bytes=40 * 2**20),
        name="finish",
    )(
        at,
        *near(factor, low),
        *far(query_basis, output_basis, query_master, output_master, gathered, gathered, gathered),
        *far(*quarters[:5]),
        *near(*quarters[5:]),
    )


def per_device(
    saved_input,
    query_cotangent,
    layer_cotangent,
    mixed_heads,
    query_basis,
    output_basis,
    query_master,
    output_master,
    query_first,
    query_second,
    output_first,
    output_second,
):
    shape = jax.ShapeDtypeStruct
    at = jnp.stack([lax.axis_index("fs_2"), lax.axis_index("tp"), lax.axis_index(FS)]).astype(jnp.int32)
    moments = (query_first, query_second, output_first, output_second)
    block, send, cot = pl.pallas_call(
        pack_kernel,
        in_specs=[SMEM] + [VMEM] * 10,
        out_specs=[VMEM] * 3,
        out_shape=[shape((BLOCK_ROWS, 512), bf16), shape((32, 64, 128), bf16), shape((256, 1024), bf16)],
        compiler_params=pltpu.CompilerParams(vmem_limit_bytes=24 * 2**20),
        name="pack",
    )(
        at,
        *far(query_basis, output_basis, query_master, output_master, *moments),
        *far(query_cotangent, mixed_heads),
    )
    gathered = lax.all_gather(block, FS, axis=0, tiled=False)
    cots = [cot] + [lax.ppermute(cot, "tp", [(i, (i + k) % 4) for i in range(4)]) for k in (2, 1, 3)]
    cots = [cots[i] for i in (0, 2, 1, 3)]
    mine = lax.all_to_all(send, CHIPS, 0, 0, tiled=True)
    theirs = swapped(mine)
    owns, others = [mine], [theirs]
    for k in range(1, 4):
        quarter = lax.ppermute(mine, "tp", [(i, (i + k) % 4) for i in range(4)])
        owns.append(quarter)
        others.append(swapped(quarter))
    quarters = owns + others
    keep, give = pl.pallas_call(
        project_kernel,
        in_specs=[SMEM] + [pl.BlockSpec(memory_space=pl.ANY)] * 2 + [VMEM] * 6,
        out_specs=[VMEM] * 2,
        scratch_shapes=[pltpu.VMEM((256, D), bf16)] * 2 + [pltpu.SemaphoreType.DMA((2,))],
        out_shape=[pltpu.VMEM((32, 32, 128), f32)] * 2,
        compiler_params=pltpu.CompilerParams(vmem_limit_bytes=20 * 2**20),
        name="project",
    )(at, *far(saved_input, layer_cotangent), *near(mine, theirs, *cots))
    pair = (keep + swapped(give.astype(f16)).astype(f32)).astype(f16)
    arrived = lax.all_to_all(pair, CHIPS, 0, 0, tiled=True)
    row = jnp.sum(arrived.astype(f32), axis=0)
    out = pl.pallas_call(
        spread_kernel,
        in_specs=[SMEM, VMEM],
        out_specs=VMEM,
        out_shape=pltpu.VMEM((128, 1, 1152), f32),
        compiler_params=pltpu.CompilerParams(vmem_limit_bytes=16 * 2**20),
        name="spread",
    )(at, *near(row))
    mine = lax.all_to_all(out, (*CHIPS, "tp"), 0, 0, tiled=True)
    theirs = swapped(mine)
    low, factor, qf, qs, of, osec = pl.pallas_call(
        update_kernel,
        in_specs=[SMEM] + [VMEM] * 6,
        out_specs=[VMEM] * 6,
        out_shape=[shape((RANK, 1024), f32), shape((8, 128), f32)] + [shape((4, 512), f32)] * 4,
        compiler_params=pltpu.CompilerParams(vmem_limit_bytes=16 * 2**20),
        name="update",
    )(at, *near(mine, theirs), *far(*moments))

    query_weight, output_weight, query_step, output_step, query_copy, output_copy = finished(
        at, factor, low, query_basis, output_basis, query_master, output_master, gathered, quarters
    )
    return (
        query_weight,
        output_weight,
        query_step,
        output_step,
        qf,
        qs,
        of,
        osec,
        query_copy,
        output_copy,
    )


def solution(mesh):
    torus = Mesh(mesh.devices.reshape(8, 4, 2, mesh.shape["tp"]), (*FS, "tp"))
    return jax.shard_map(
        per_device,
        mesh=torus,
        in_specs=(
            P(FS, None),
            P(FS, "tp"),
            P(FS, None),
            P(FS, "tp"),
            P(FS, None),
            P(FS, None),
            *[P(FS, "tp")] * 6,
        ),
        out_specs=(*[P(FS, "tp")] * 8, P(None, "tp"), P(None, "tp")),
        check_vma=False,
    )
```

```python
import jax
import jax.numpy as jnp
from jax import lax
from jax.experimental import pallas as pl
from jax.experimental.pallas import tpu as pltpu
from jax.sharding import Mesh
from jax.sharding import PartitionSpec as P

D = 4096
QW = 2048
RANK = 256
FS = ("fs_0", "fs_1", "fs_2")
CHIPS = ("fs_0", "fs_1")

beta_one = 0.8
beta_two = 0.9
rate = 0.1

f32 = jnp.float32
bf16 = jnp.bfloat16
f16 = jnp.float16

REACH = 85.0
SHRINK = 2.0**-10

MOMENTS_AT = 128
TOPS_AT = 144
BLOCK_ROWS = 152
GROUP = 16


VMEM = pl.BlockSpec(memory_space=pltpu.VMEM)
SMEM = pl.BlockSpec(memory_space=pltpu.SMEM)


def high_and_low(values):
    high = values.astype(bf16).astype(f32)
    return high, values - high


def coded(values):
    top = jnp.max(jnp.abs(values), axis=(0, 1), keepdims=True) * 1.01 + 1e-30
    top = top.astype(bf16).astype(f32)
    return jnp.exp(values * (REACH / top)), top


def pack_kernel(at, qb, ob, qm, om, q1, q2, o1, o2, qc, oc, block, send, cot):
    tp = at[1]
    picked = []
    for basis in (qb, ob):
        full = basis[...].astype(f32)
        part = full[:, :64]
        for t in range(1, 4):
            part = jnp.where(tp == t, full[:, 64 * t : 64 * t + 64], part)
        picked.append(part)
    send[...] = jnp.broadcast_to(jnp.concatenate(picked, axis=1).astype(bf16)[None], send.shape)
    row = lax.broadcasted_iota(jnp.int32, (8, 512), 0)
    tops = jnp.zeros((8, 512), f32)
    for side, master in ((0, qm), (1, om)):
        codes, top = coded(master[...])
        block[64 * side : 64 * side + 64, :] = codes.astype(bf16)
        tops = jnp.where(row == side, top, tops)
    held = []
    for side, first, second in ((0, q1, q2), (1, o1, o2)):
        for at_row, values in ((2 + side, first), (4 + side, second)):
            codes, top = coded(values[...])
            held.append(codes)
            tops = jnp.where(row == at_row, top, tops)
    block[MOMENTS_AT : MOMENTS_AT + 16, :] = jnp.concatenate(held, axis=0).astype(bf16)
    block[TOPS_AT:, :] = tops.astype(bf16)
    cot[:, :512] = qc[...]
    cot[:, 512:] = oc[...]


def project_kernel(at, saved, layer, mine, theirs, c0, c1, c2, c3, keep, give, saved_near, layer_near, sems):
    copies = [
        pltpu.make_async_copy(saved, saved_near, sems.at[0]),
        pltpu.make_async_copy(layer, layer_near, sems.at[1]),
    ]
    for copy in copies:
        copy.start()
    core = at[0]
    own, other = mine[...], theirs[...]
    first = jnp.where(core == 0, own, other)
    second = jnp.where(core == 0, other, own)
    basis = jnp.concatenate([first, second], axis=1).reshape(D, 128)
    for side, source in ((0, saved_near), (1, layer_near)):
        copies[side].wait()
        coords = jnp.dot(source[...], basis, preferred_element_type=f32)[:, 64 * side : 64 * side + 64]
        high, low = high_and_low(coords.T)
        left = jnp.concatenate([high, low], axis=0).astype(bf16)
        for k, cot in enumerate((c0, c1, c2, c3)):
            both = jnp.dot(left, cot[:, 512 * side : 512 * side + 512], preferred_element_type=f32)
            part = (both[:64] + both[64:]) * SHRINK
            lower, upper = part[:32], part[32:]
            kept = jnp.where(core == 0, lower, upper)
            given = jnp.where(core == 0, upper, lower)
            for j in range(4):
                slot = (side * 4 + k) * 4 + j
                keep[:, slot, :] = kept[:, 128 * j : 128 * j + 128]
                give[:, slot, :] = given[:, 128 * j : 128 * j + 128]


def spread_kernel(at, row, out):
    tp = at[1]
    values = row[...] * (1.0 / SHRINK)
    squares = jnp.broadcast_to(jnp.sum(values * values, axis=(0, 1), keepdims=True), (1, 128))
    for t in range(4):
        k = (tp + 4 - t) % 4
        pieces = []
        for side in range(2):
            for j in range(4):
                pieces.append(row[pl.ds((side * 4 + k) * 4 + j, 1), :] * (1.0 / SHRINK))
        line = jnp.concatenate(pieces + [squares], axis=1)

        def put(chip, carry):
            out[chip * 4 + t] = line
            return carry

        lax.fori_loop(0, 32, put, 0, unroll=True)


def update_kernel(at, mine, theirs, q1, q2, o1, o2, low, factor, qf, qs, of, os):
    core, fs = at[0], at[2]
    total = jnp.sum(mine[:, :, 1024:], axis=0) + jnp.sum(theirs[:, :, 1024:], axis=0)
    scale = lax.rsqrt(1.0 + total * (1.0 / (2.0 * RANK * QW)))
    factor[...] = jnp.broadcast_to(scale, (8, 128))
    is_first = core == 0
    for t in range(4):
        for chip in range(32):
            own, other = mine[chip * 4 + t, :, :1024], theirs[chip * 4 + t, :, :1024]
            low[64 * t + chip : 64 * t + chip + 1, :] = jnp.where(is_first, own, other)
            low[64 * t + 32 + chip : 64 * t + 33 + chip, :] = jnp.where(is_first, other, own)
    near = low[pl.ds(pl.multiple_of(fs // 2 * 8, 8), 8), :]
    own_rows = jnp.where(fs % 2 == 0, near[:4], near[4:]) * scale[:, :1]
    for side, first, second, first_new, second_new in ((0, q1, q2, qf, qs), (1, o1, o2, of, os)):
        scaled = own_rows[:, 512 * side : 512 * side + 512]
        first_new[...] = beta_one * first[...] + (1.0 - beta_one) * scaled
        second_new[...] = beta_two * second[...] + (1.0 - beta_two) * scaled * scaled


def finish_kernel(
    at, factor, low, qb, ob, qm, om, moments, gathered, tops, *rest
):
    quarters, (qw, ow, qs, os, qc, oc, natural, direction, held_codes, sems) = rest[:8], rest[8:]
    core, tp = at[0], at[1]
    step, steps = pl.program_id(0), 64 // GROUP

    def fetch(i):
        source = gathered.at[pl.ds(i * GROUP, GROUP), pl.ds(0, 128), :]
        return pltpu.make_async_copy(source, held_codes.at[i % 2], sems.at[i % 2])

    @pl.when(step == 0)
    def _():
        fetch(0).start()

    @pl.when(step + 1 < steps)
    def _():
        fetch(step + 1).start()

    @pl.when(pl.program_id(0) == 0)
    def _():
        scale = factor[0:1, 0:1]

        is_first = lax.broadcasted_iota(jnp.int32, (8, 512), 0) < 4

        def rows(i, carry):
            codes = moments[pl.ds(4 * i, 4)].astype(f32)
            units = tops[pl.ds(4 * i, 4)].astype(f32) * (1.0 / REACH)
            lows = low[pl.ds(16 * i, 16), :] * scale
            for side in range(2):
                held = []
                for j in range(4):
                    unit = jnp.where(is_first, units[j, 2 + side : 3 + side], units[j, 4 + side : 5 + side])
                    held.append(jnp.log(codes[j, 8 * side : 8 * side + 8]) * unit)
                first = jnp.concatenate([h[:4] for h in held], axis=0)
                second = jnp.concatenate([h[4:] for h in held], axis=0)
                scaled = lows[:, 512 * side : 512 * side + 512]
                first = beta_one * first + (1.0 - beta_one) * scaled
                second = beta_two * second + (1.0 - beta_two) * scaled * scaled
                natural[pl.ds(16 * i, 16), 512 * side : 512 * side + 512] = (first / jnp.sqrt(second)).astype(bf16)
            return carry

        lax.fori_loop(0, 16, rows, 0, unroll=4)
        for k in range(4):
            start = pl.multiple_of((tp + 4 - k) % 4 * 64, 64)
            direction[64 * k : 64 * k + 64, :] = natural[pl.ds(start, 64), :]
        for side, basis, master, weight, step in ((0, qb, qm, qw, qs), (1, ob, om, ow, os)):
            moved = jnp.dot(basis[...], natural[:, 512 * side : 512 * side + 512], preferred_element_type=f32)
            step[...] = moved
            weight[...] = master[...] - rate * moved

    fetch(step).wait()
    block = held_codes.at[step % 2]
    bases = []
    for k in range(4):
        chips = pl.ds(pl.program_id(0) * (GROUP // 2), GROUP // 2)
        own, other = quarters[k][...], quarters[4 + k][chips]
        first = jnp.where(core == 0, own, other)
        second = jnp.where(core == 0, other, own)
        bases.append(jnp.concatenate([first, second], axis=1).reshape(GROUP * 64, 128))
    for side, copy in ((0, qc), (1, oc)):
        basis = jnp.concatenate([b[:, 64 * side : 64 * side + 64] for b in bases], axis=1)
        moved = jnp.dot(basis, direction[:, 512 * side : 512 * side + 512], preferred_element_type=f32)
        codes = block[:, 64 * side : 64 * side + 64, :].astype(f32)
        blocks = pl.ds(pl.program_id(0) * GROUP, GROUP)
        unit = tops[blocks, side : side + 1, :].astype(f32) * (1.0 / REACH)
        master = (jnp.log(codes) * unit).reshape(GROUP * 64, 512)
        copy[...] = (master - rate * moved).astype(bf16)


def near(*arrays):
    return [pltpu.with_memory_space_constraint(a, pltpu.VMEM) for a in arrays]


def far(*arrays):
    return [pltpu.with_memory_space_constraint(a, pltpu.HBM) for a in arrays]


def swapped(values):
    return lax.ppermute(values, "fs_2", [(0, 1), (1, 0)])


def finished(at, factor, low, query_basis, output_basis, query_master, output_master, gathered, quarters):
    shape = jax.ShapeDtypeStruct

    def whole(*dims):
        return pl.BlockSpec(dims, lambda i: (0,) * len(dims))

    local = whole(64, 512)
    return pl.pallas_call(
        finish_kernel,
        grid=(64 // GROUP,),
        in_specs=[
            SMEM,
            whole(8, 128),
            whole(RANK, 1024),
            whole(64, 256),
            whole(64, 256),
            local,
            local,
            pl.BlockSpec((64, 16, 512), lambda i: (0, MOMENTS_AT // 16, 0)),
            pl.BlockSpec(memory_space=pl.ANY),
            pl.BlockSpec((64, 8, 512), lambda i: (0, TOPS_AT // 8, 0)),
            *[pl.BlockSpec((GROUP // 2, 64, 128), lambda i: (i, 0, 0))] * 4,
            *[VMEM] * 4,
        ],
        out_specs=[local] * 4 + [pl.BlockSpec((GROUP * 64, 512), lambda i: (i, 0))] * 2,
        out_shape=[shape((64, 512), f32)] * 4 + [shape((D, 512), bf16)] * 2,
        scratch_shapes=[pltpu.VMEM((RANK, 1024), bf16)] * 2
        + [pltpu.VMEM((2, GROUP, 128, 512), bf16), pltpu.SemaphoreType.DMA((2,))],
        compiler_params=pltpu.CompilerParams(dimension_semantics=("arbitrary",), vmem_limit_bytes=40 * 2**20),
        name="finish",
    )(
        at,
        *near(factor, low),
        *far(query_basis, output_basis, query_master, output_master, gathered, gathered, gathered),
        *far(*quarters[:4]),
        *near(*quarters[4:]),
    )


def per_device(
    saved_input,
    query_cotangent,
    layer_cotangent,
    mixed_heads,
    query_basis,
    output_basis,
    query_master,
    output_master,
    query_first,
    query_second,
    output_first,
    output_second,
):
    shape = jax.ShapeDtypeStruct
    at = jnp.stack([lax.axis_index("fs_2"), lax.axis_index("tp"), lax.axis_index(FS)]).astype(jnp.int32)
    moments = (query_first, query_second, output_first, output_second)
    block, send, cot = pl.pallas_call(
        pack_kernel,
        in_specs=[SMEM] + [VMEM] * 10,
        out_specs=[VMEM] * 3,
        out_shape=[shape((BLOCK_ROWS, 512), bf16), shape((32, 64, 128), bf16), shape((256, 1024), bf16)],
        compiler_params=pltpu.CompilerParams(vmem_limit_bytes=24 * 2**20),
        name="pack",
    )(
        at,
        *far(query_basis, output_basis, query_master, output_master, *moments),
        *far(query_cotangent, mixed_heads),
    )
    gathered = lax.all_gather(block, FS, axis=0, tiled=False)
    cots = [cot] + [lax.ppermute(cot, "tp", [(i, (i + k) % 4) for i in range(4)]) for k in (2, 1, 3)]
    cots = [cots[i] for i in (0, 2, 1, 3)]
    mine = lax.all_to_all(send, CHIPS, 0, 0, tiled=True)
    theirs = swapped(mine)
    owns, others = [mine], [theirs]
    for k in range(1, 4):
        quarter = lax.ppermute(mine, "tp", [(i, (i + k) % 4) for i in range(4)])
        owns.append(quarter)
        others.append(swapped(quarter))
    quarters = owns + others
    keep, give = pl.pallas_call(
        project_kernel,
        in_specs=[SMEM] + [pl.BlockSpec(memory_space=pl.ANY)] * 2 + [VMEM] * 6,
        out_specs=[VMEM] * 2,
        scratch_shapes=[pltpu.VMEM((256, D), bf16)] * 2 + [pltpu.SemaphoreType.DMA((2,))],
        out_shape=[pltpu.VMEM((32, 32, 128), f32)] * 2,
        compiler_params=pltpu.CompilerParams(vmem_limit_bytes=20 * 2**20),
        name="project",
    )(at, *far(saved_input, layer_cotangent), *near(mine, theirs, *cots))
    pair = (keep + swapped(give.astype(f16)).astype(f32)).astype(f16)
    arrived = lax.all_to_all(pair, CHIPS, 0, 0, tiled=True)
    row = jnp.sum(arrived.astype(f32), axis=0)
    out = pl.pallas_call(
        spread_kernel,
        in_specs=[SMEM, VMEM],
        out_specs=VMEM,
        out_shape=pltpu.VMEM((128, 1, 1152), f32),
        compiler_params=pltpu.CompilerParams(vmem_limit_bytes=16 * 2**20),
        name="spread",
    )(at, *near(row))
    mine = lax.all_to_all(out, (*CHIPS, "tp"), 0, 0, tiled=True)
    theirs = swapped(mine)
    low, factor, qf, qs, of, osec = pl.pallas_call(
        update_kernel,
        in_specs=[SMEM] + [VMEM] * 6,
        out_specs=[VMEM] * 6,
        out_shape=[shape((RANK, 1024), f32), shape((8, 128), f32)] + [shape((4, 512), f32)] * 4,
        compiler_params=pltpu.CompilerParams(vmem_limit_bytes=16 * 2**20),
        name="update",
    )(at, *near(mine, theirs), *far(*moments))

    query_weight, output_weight, query_step, output_step, query_copy, output_copy = finished(
        at, factor, low, query_basis, output_basis, query_master, output_master, gathered, quarters
    )
    return (
        query_weight,
        output_weight,
        query_step,
        output_step,
        qf,
        qs,
        of,
        osec,
        query_copy,
        output_copy,
    )


def solution(mesh):
    torus = Mesh(mesh.devices.reshape(8, 4, 2, mesh.shape["tp"]), (*FS, "tp"))
    return jax.shard_map(
        per_device,
        mesh=torus,
        in_specs=(
            P(FS, None),
            P(FS, "tp"),
            P(FS, None),
            P(FS, "tp"),
            P(FS, None),
            P(FS, None),
            *[P(FS, "tp")] * 6,
        ),
        out_specs=(*[P(FS, "tp")] * 8, P(None, "tp"), P(None, "tp")),
        check_vma=False,
    )
```
